32 devices in a mesh: ep: 16 (over z, y, x), tp: 2 (over core).
Axes of the slice: x: 2, y: 2, z: 4, core: 2. Of those that a mesh axis runs over, the one named last changes fastest.
Arguments:
- tokens: bfloat16 [4096, 2048], P('ep'), may hold values from -6 to 6
- expert_ids: int32 [4096, 4], P('ep'), may hold values from 0 to 15, all different within a row; in each aligned block of 256 rows (0 to 255, 256 to 511, ...) at most 96 rows name the same one
- gates: float32 [4096, 4], P('ep'), may hold values from 0.05 to 0.6
- cotangent: bfloat16 [4096, 2048], P('ep'), may hold values from -6 to 6
- w_gate: bfloat16 [16, 2048, 512], P('ep', None, 'tp'), may hold values from -0.125 to 0.125
- w_up: bfloat16 [16, 2048, 512], P('ep', None, 'tp'), may hold values from -0.125 to 0.125
- w_down: bfloat16 [16, 512, 2048], P('ep', 'tp'), may hold values from -0.25 to 0.25
- sh_gate: bfloat16 [2048, 512], P(None, 'tp'), may hold values from -0.125 to 0.125
- sh_up: bfloat16 [2048, 512], P(None, 'tp'), may hold values from -0.125 to 0.125
- sh_down: bfloat16 [512, 2048], P('tp'), may hold values from -0.25 to 0.25
Outputs:
- token_grad: bfloat16 [4096, 2048], P('ep', 'tp')
- gate_grad: float32 [4096, 4], P('ep')
- expert_gate_grad: float32 [16, 2048, 512], P('ep', None, 'tp')
- expert_up_grad: float32 [16, 2048, 512], P('ep', None, 'tp')
- expert_down_grad: float32 [16, 512, 2048], P('ep', 'tp')
- shared_gate_grad: float32 [2048, 512], P('ep', 'tp')
- shared_up_grad: float32 [2048, 512], P('ep', 'tp')
- shared_down_grad: float32 [512, 2048], P('tp', 'ep')
- expert_gate_rows: float32 [16, 2048], P('ep')
- expert_up_rows: float32 [16, 2048], P('ep')
- expert_down_rows: float32 [16, 512], P('ep', 'tp')
- shared_gate_rows: float32 [2048], P('ep')
- shared_up_rows: float32 [2048], P('ep')
- shared_down_rows: float32 [512], P('tp')
The draws below stay inside these ranges and needn't reach their ends.
Inputs may be any that keep to these rules, and one draw needn't show every extreme that they name: `expert_ids`: each row names 4 different experts. Within each aligned block of 256 tokens no expert is named by more than 96 assignments, a bound that is reached in some blocks.
All inputs are finite; a program needn't handle non-finite values.
Results may differ from the reference program's by a relative error of at most 0.0085.
Values may be sent and summed in bfloat16 or wider, within the bound.
A program may use at most 128 MiB of HBM per device.

```python
import math
import jax
import jax.numpy as jnp
import numpy as np
from jax import lax

D = 2048
HID = 512
SH = 512
TOP_K = 4
TOK_DEV = 256
EXPERTS = 16
CAP = 96
TOKENS = 4096
N_TP = 2


def with_spikes(values, stream_key, source, target, parts, factor):
    def block_of(position):
        return (jnp.arange(values.shape[position]) // (values.shape[position] // parts)).reshape((-1,) + (1,) * (values.ndim - 1 - position))

    first = jax.random.permutation(stream_key, parts)[block_of(target)]
    second = (block_of(target) + parts // 2) % parts
    return jnp.where((block_of(source) == first) | (block_of(source) == second), factor * values, values)


def levels(stream_key, shape, split, least, high):
    def one(dim, shards_of):
        steps = jax.random.uniform(jax.random.fold_in(jax.random.fold_in(stream_key, 6), dim), (shards_of,), jnp.float32, least / len(split), high / len(split))
        return jnp.repeat(jnp.exp(steps), shape[dim] // shards_of).reshape((-1,) + (1,) * (len(shape) - dim - 1))

    loudness = one(*split[0])
    for cut in split[1:]:
        loudness = loudness * one(*cut)
    return loudness


def deal_out(stream_key, own, number, rows, amount, top, reach, skew):
    ranking = jax.random.permutation(stream_key, amount)
    crowded, ordinary = load_shares(amount, rows * top, reach, skew, True), load_shares(amount, rows * top, reach, skew, False)
    places = jnp.arange(amount)

    def named(sizes, offset_by):
        used = int((sizes > 0).sum())
        fixed = max(1, used // 4)
        passed = fixed + (places - fixed + offset_by * (used - fixed)) % max(1, amount - fixed)
        return jnp.zeros((amount,), jnp.int32).at[ranking[jnp.where(places < fixed, places, passed)]].set(jnp.asarray(sizes, jnp.int32))

    sizes = jnp.where(number % 4 == 0, named(crowded, number // 4), named(ordinary, number - number // 4 - 1))
    mixed = jax.random.permutation(jax.random.fold_in(own, 3), amount)
    giver, sink = mixed[0:amount // 2 * 2:2], mixed[1:amount // 2 * 2:2]
    room = jnp.minimum(sizes[giver] - 1, reach - sizes[sink]) // 2
    room = jnp.where((giver == ranking[0]) | (sink == ranking[0]) | (sizes[sink] == 0), 0, jnp.maximum(room, 0))
    passed = jax.random.randint(jax.random.fold_in(own, 4), (amount // 2,), 0, 1 << 20) % (room + 1)
    sizes = sizes.at[giver].add(-passed).at[sink].add(passed)
    members = jnp.searchsorted(jnp.cumsum(sizes), jnp.arange(rows * top), side="right").astype(jnp.int32)
    grid = members.reshape(top, rows).T
    grid = grid[jax.random.permutation(jax.random.fold_in(own, 1), rows)]
    offset_by = jax.random.randint(jax.random.fold_in(own, 2), (rows, 1), 0, top)
    return jnp.take_along_axis(grid, (jnp.arange(top)[None, :] + offset_by) % top, axis=1)


def load_shares(count, total, most, skew, full):
    weights = [(1 << 20) // math.isqrt(grade ** skew) + 1 for grade in range(1, count + 1)]
    largest = most if full else min(most, max(-(-total // count), total * weights[0] // sum(weights)))
    least = 1 if total - largest >= count - 1 else 0
    given, spare = [largest] + [least] * (count - 1), total - largest - least * (count - 1)
    while spare > 0:
        movable = [i for i in range(1, count) if given[i] < largest] or [i for i in range(1, count) if given[i] < most]
        mass, remaining = sum([weights[i] for i in movable]), spare
        for i in movable:
            addition = min(most - given[i], max(1, remaining * weights[i] // mass), spare)
            given[i] = given[i] + addition
            spare = spare - addition
    return np.array(given)


def bell_draw(key, shape, deviation, reach, shards=(), kind=jnp.bfloat16):
    array = deviation * jax.random.normal(key, shape, jnp.float32)
    if shards:
        array = array * levels(key, shape, shards, -0.22, 0.18)
    return jnp.clip(array, -reach, reach).astype(kind)


def noise_with(key, extent, deviation, bound, cuts, heavy, kind=jnp.bfloat16):
    values = deviation * jax.random.normal(key, extent, jnp.float32)
    if cuts:
        values = values * levels(key, extent, cuts, -0.22, 0.18)
    return jnp.clip(with_spikes(values, jax.random.fold_in(key, 3), *heavy), -bound, bound).astype(kind)


def setup_inputs(seed: int = 0) -> dict:
    keys = jax.random.split(jax.random.key(seed), 11)
    tokens = noise_with(keys[0], (TOKENS, D), 1.0, 6.0, ((0, 16),), (0, 1, 16, 2.0))
    expert_ids_keys = jax.random.split(jax.random.fold_in(keys[1], 1), TOKENS // TOK_DEV)
    expert_ids_turns = jax.random.permutation(jax.random.fold_in(keys[1], 3), TOKENS // TOK_DEV)
    expert_ids = jax.vmap(lambda own, number: deal_out(jax.random.fold_in(keys[1], 2), own, number, TOK_DEV, EXPERTS, TOP_K, CAP, 2))(expert_ids_keys, expert_ids_turns).reshape((TOKENS, TOP_K))
    gates = jnp.clip(0.05 + 0.55 * jax.random.uniform(keys[2], (TOKENS, TOP_K), jnp.float32) ** levels(keys[2], (TOKENS, TOP_K), ((0, 16),), -0.2, 0.2), 0.05, 0.6)
    cotangent = noise_with(keys[3], (TOKENS, D), 1.0, 6.0, ((0, 16),), (0, 1, 16, 2.0))
    w_gate = bell_draw(keys[4], (EXPERTS, D, HID), D ** -0.5, 0.125, ((0, 16), (2, 2)))
    w_up = bell_draw(keys[5], (EXPERTS, D, HID), D ** -0.5, 0.125, ((0, 16), (2, 2)))
    w_down = bell_draw(keys[6], (EXPERTS, HID, D), HID ** -0.5, 0.25, ((0, 16), (1, 2)))
    sh_gate = bell_draw(keys[7], (D, SH), D ** -0.5, 0.125, ((1, 2),))
    sh_up = bell_draw(keys[8], (D, SH), D ** -0.5, 0.125, ((1, 2),))
    sh_down = bell_draw(keys[9], (SH, D), SH ** -0.5, 0.25, ((0, 2),))
    return dict(tokens=tokens, expert_ids=expert_ids, gates=gates, cotangent=cotangent, w_gate=w_gate, w_up=w_up, w_down=w_down, sh_gate=sh_gate, sh_up=sh_up, sh_down=sh_down)


def silu_parts(pre):
    sigmoid = jax.nn.sigmoid(pre)
    return pre * sigmoid, sigmoid * (1.0 + pre * (1.0 - sigmoid))


def halves_sum(left_a, right_a, left_b, right_b, pieces):
    step_cols = left_a.shape[1] // pieces
    total = jnp.zeros((left_a.shape[0], right_a.shape[0]), jnp.float32)
    for piece in range(pieces):
        first_col = piece * step_cols
        part = jnp.dot(left_a[:, first_col:first_col + step_cols], right_a[:, first_col:first_col + step_cols].T, preferred_element_type=jnp.float32)
        part = part + jnp.dot(left_b[:, first_col:first_col + step_cols], right_b[:, first_col:first_col + step_cols].T, preferred_element_type=jnp.float32)
        total = total + lax.optimization_barrier(part.astype(jnp.bfloat16)).astype(jnp.float32)
    return total


def backward_rows(inputs, cot_rows, w_g, w_u, w_d):
    gate_pre = jnp.dot(inputs, w_g, preferred_element_type=jnp.float32)
    up_pre = jnp.dot(inputs, w_u, preferred_element_type=jnp.float32)
    active, slope = silu_parts(gate_pre)
    hidden = (active * up_pre).astype(jnp.bfloat16)
    hidden_cot = jnp.dot(cot_rows, w_d.T, preferred_element_type=jnp.float32)
    gate_sum = jnp.sum(hidden.astype(jnp.float32) * hidden_cot, axis=1)
    d_gate = (hidden_cot * up_pre * slope).astype(jnp.bfloat16)
    d_up = (hidden_cot * active).astype(jnp.bfloat16)
    grad_g = jnp.dot(inputs.T, d_gate, preferred_element_type=jnp.float32)
    grad_u = jnp.dot(inputs.T, d_up, preferred_element_type=jnp.float32)
    grad_d = jnp.dot(hidden.T, cot_rows, preferred_element_type=jnp.float32)
    rows = halves_sum(d_gate, w_g, d_up, w_u, N_TP)
    return grad_g, grad_u, grad_d, rows, gate_sum


def reference(tokens, expert_ids, gates, cotangent, w_gate, w_up, w_down, sh_gate, sh_up, sh_down):
    per_dev = TOK_DEV * TOP_K
    assign = TOKENS * TOP_K
    slots = EXPERTS * CAP
    flat_ids = expert_ids.reshape(EXPERTS, per_dev).astype(jnp.int32)
    onehot = (flat_ids[:, :, None] == jnp.arange(EXPERTS, dtype=jnp.int32)[None, None, :]).astype(jnp.int32)
    slot_rank = jnp.sum((jnp.cumsum(onehot, axis=1) - 1) * onehot, axis=2)
    sources = jnp.arange(EXPERTS, dtype=jnp.int32)[:, None]
    slot_row = (flat_ids * slots + sources * CAP + slot_rank).reshape(assign).astype(jnp.int32)
    slot_table = jnp.full((EXPERTS * slots,), assign, jnp.int32).at[slot_row].set(jnp.arange(assign, dtype=jnp.int32))
    filled = slot_table < assign
    source = jnp.minimum(slot_table, assign - 1)
    token_row = (source // TOP_K).astype(jnp.int32)
    slot_gate = jnp.where(filled, gates.reshape(assign)[source], jnp.zeros((), jnp.float32))

    def one_expert(packed):
        rows_index, gate_col, keep, w_g, w_u, w_d = packed
        inputs = jnp.where(keep[:, None], tokens[rows_index], jnp.zeros((), tokens.dtype))
        cot_rows = (gate_col[:, None] * cotangent[rows_index].astype(jnp.float32)).astype(jnp.bfloat16)
        return backward_rows(inputs, cot_rows, w_g, w_u, w_d)

    grad_g, grad_u, grad_d, slot_rows, gate_sums = lax.map(one_expert, (token_row.reshape(EXPERTS, slots), slot_gate.reshape(EXPERTS, slots), filled.reshape(EXPERTS, slots), w_gate, w_up, w_down))
    flat_rows = slot_rows.reshape(EXPERTS * slots, D)
    picks = slot_row.reshape(TOKENS, TOP_K)
    routed = jnp.zeros((TOKENS, D), jnp.float32)
    for column in range(TOP_K):
        routed = routed + flat_rows[picks[:, column]].astype(jnp.float32)
    gate_grad = gate_sums.reshape(EXPERTS * slots)[picks] / gates
    shared_g, shared_u, shared_d, shared_rows, unused = backward_rows(tokens, cotangent, sh_gate, sh_up, sh_down)
    token_grad = (routed + shared_rows).astype(jnp.bfloat16)
    return (token_grad, gate_grad, grad_g, grad_u, grad_d, shared_g, shared_u, shared_d,
            jnp.sum(grad_g * grad_g, axis=2), jnp.sum(grad_u * grad_u, axis=2), jnp.sum(grad_d * grad_d, axis=2),
            jnp.sum(shared_g * shared_g, axis=1), jnp.sum(shared_u * shared_u, axis=1), jnp.sum(shared_d * shared_d, axis=1))
```

```python
import functools
import math

import jax
import jax.numpy as jnp
from jax import lax
from jax.experimental import pallas as pl
from jax.experimental.pallas import tpu as pltpu
from jax.sharding import PartitionSpec as P

BF16 = jnp.bfloat16
F32 = jnp.float32
LAST = (((1,), (1,)), ((), ()))
FIRST = (((0,), (0,)), ((), ()))


def silu_parts(pre):
    sigmoid = jax.nn.sigmoid(pre)
    return (pre * sigmoid, sigmoid * (1.0 + pre * (1.0 - sigmoid)))


def dot(left, right):
    return jnp.dot(left, right, preferred_element_type=F32)


def dot_last(left, right):
    return lax.dot_general(left, right, LAST, preferred_element_type=F32)


def dot_first(left, right):
    return lax.dot_general(left, right, FIRST, preferred_element_type=F32)


def row_sums(values):
    ones = jnp.ones((8, values.shape[1]), F32)
    sums = lax.dot_general(
        ones, values, LAST, precision=lax.Precision.HIGHEST, preferred_element_type=F32
    )
    return sums[:1]


def plane_count(mesh):
    count = mesh.shape["ep"]
    try:
        planes = len({tuple(d.coords)[2] for d in mesh.devices.flat})
    except (AttributeError, TypeError, IndexError):
        planes = 0
    if planes < 1 or count % planes:
        planes = max(d for d in range(1, math.isqrt(count) + 1) if count % d == 0)
    return planes


def copy_to(src, dst, send, recv, ep, tp):
    return pltpu.make_async_remote_copy(
        src_ref=src,
        dst_ref=dst,
        send_sem=send,
        recv_sem=recv,
        device_id=(ep, tp),
        device_id_type=pl.DeviceIdType.MESH,
    )


def layer_kernel(
    planes, width, cap,
    table, tokens, cotangent, wg_in, wu_in, wd_in, sg_in, su_in, sd_in,
    tok_out, gg_out, gu_out, gd_out, sg_out, su_out, sd_out, norm_out, down_out, sdn_out, gate_out,
    toks, cots, line_table, ready, land_t, land_c,
    w_g, w_u, w_d, s_g, s_u, s_d,
    hid, dgate, dup, tp_in, ret_in, z_out, z_in, routed,
    stage_g, stage_u, stage_d, acc_g, acc_u, acc_d,
    deal_gu, deal_d, deal_gu_in, deal_d_in, sh_part, sh_in,
    gate_part, gate_in, gate_sum, norm_part, norm_in, sdn_part,
    load_sem, table_sem, line_sem, share_sem, plane_sem, pair_sem, tp_sem, ret_sem, z_sem,
    deal_sem, misc_sem, gate_sem, sdn_sem, stage_sem,
):
    me, core = lax.axis_index("ep"), lax.axis_index("tp")
    z, q = me // width, me % width
    experts = planes * width
    rows, model = tokens.shape
    cols = model // 2
    hidden = w_g.shape[1]
    slots = width * cap
    take = model // experts
    span = width * take
    mine = pl.ds(pl.multiple_of(core * cols, cols), cols)
    other = pl.ds(pl.multiple_of((1 - core) * cols, cols), cols)
    parts = (toks, cots)
    lands = (land_t, land_c)

    def landed(ref, sem):
        copy_to(ref, ref, sem, sem, me, 1 - core).wait_recv()

    def sent(ref, sem):
        copy_to(ref, ref, sem, sem, me, 1 - core).wait_send()

    loads = [
        pltpu.make_async_copy(src, dst, load_sem.at[i])
        for i, (src, dst) in enumerate(
            (
                (tokens, toks.at[z]),
                (cotangent, cots.at[z]),
                (sg_in, s_g),
                (su_in, s_u),
                (sd_in, s_d),
                (wg_in, w_g),
                (wu_in, w_u),
                (wd_in, w_d),
            )
        )
    ]
    for load in loads:
        load.start()

    def table_copy(step):
        peer = (z + step) % planes * width + q
        return copy_to(
            table, line_table.at[z], table_sem.at[0, step - 1], table_sem.at[1, step - 1], peer, core
        )

    for step in range(1, planes):
        table_copy(step).start()
    line_table[z] = table[...]

    def line_copy(way, block, part):
        there = jnp.clip(z + 1 - 2 * way, 0, planes - 1)
        ref = parts[part].at[block, :, mine]
        return copy_to(
            ref, ref, line_sem.at[0, way, block, part], line_sem.at[1, way, block, part],
            there * width + q, core,
        )

    def onward(way):
        there = z + 1 - 2 * way
        return (there >= 0) & (there < planes)

    def share_copy(block, part):
        ref = parts[part].at[block, :, mine]
        return copy_to(ref, ref, share_sem.at[0, block, part], share_sem.at[1, block, part], me, 1 - core)

    def plane_copy(block, d, part):
        to_q = (q + d) % width
        return copy_to(
            ready.at[block, part, to_q],
            lands[part].at[block, q, :, mine],
            plane_sem.at[0, block, d, part],
            plane_sem.at[1, block, d, part],
            z * width + to_q,
            core,
        )

    def pair_copy(block, d, part):
        ref = lands[part].at[block, (q + width - d) % width, :, mine]
        return copy_to(
            ref, ref, pair_sem.at[0, block, d, part], pair_sem.at[1, block, d, part], me, 1 - core
        )

    def tp_copy(block):
        return copy_to(
            ready.at[block, 1 - core], tp_in.at[block], tp_sem.at[0, block], tp_sem.at[1, block],
            me, 1 - core,
        )

    def ret_copy(block, d):
        to_q = (q + d) % width
        return copy_to(
            tp_in.at[block, to_q], ret_in.at[block, q], ret_sem.at[0, block, d], ret_sem.at[1, block, d],
            z * width + to_q, core,
        )

    def z_copy(block):
        return copy_to(
            z_out.at[block], z_in.at[z], z_sem.at[0, block], z_sem.at[1, z], block * width + q, core
        )

    def hits(block):
        ranks = line_table[block, 0, z]
        at = lax.broadcasted_iota(jnp.int32, (width, cap, rows), 1).astype(F32)
        return (at == ranks).reshape(slots, rows)

    def each(step, act):
        def one(way, carry):
            block = z - step + 2 * step * way
            valid = (step >= 0) & (block >= 0) & (block < planes) & ((step > 0) | (way == 0))

            @pl.when(valid)
            def _():
                act(jnp.clip(block, 0, planes - 1), way)

            return carry

        lax.fori_loop(0, 2, one, 0)

    def select(part, block):
        hit = hits(block)
        picked = dot(jnp.where(hit, 1.0, 0.0).astype(BF16), parts[part][block, :, mine])
        if part == 1:
            gates = line_table[block, 1, z]
            gates = jnp.broadcast_to(gates, (width, cap, rows)).reshape(slots, rows)
            picked = picked * jnp.sum(jnp.where(hit, gates, 0.0), axis=1, keepdims=True)
        ready[block, part] = picked.astype(BF16).reshape(width, cap, cols)

        def one(d, carry):
            plane_copy(block, d, part).start()
            return carry

        lax.fori_loop(1, width, one, 0)
        lands[part][block, q, :, mine] = ready[block, part, q]
        pair_copy(block, 0, part).start()

    def pass_on(block, way):
        for part in range(2):

            def one(d, carry):
                landed(lands[part].at[block, q, :, mine], plane_sem.at[1, block, d, part])
                pair_copy(block, d, part).start()
                return carry

            lax.fori_loop(1, width, one, 0)

    def shared(block, way):
        for part in range(2):

            @pl.when(block != z)
            def _():
                landed(parts[part].at[block, :, other], share_sem.at[1, block, part])

        gate_pre = dot(toks[block], s_g[...])
        up_pre = dot(toks[block], s_u[...])
        active, slope = silu_parts(gate_pre)
        h = (active * up_pre).astype(BF16)
        h_cot = dot_last(cots[block], s_d[...])
        d_gate = (h_cot * up_pre * slope).astype(BF16)
        d_up = (h_cot * active).astype(BF16)
        here = pl.ds(pl.multiple_of(z * span, span), span)
        acc_g[...] += dot_first(toks[block, :, here], d_gate)
        acc_u[...] += dot_first(toks[block, :, here], d_up)
        acc_d[...] += dot_first(h, cots[block, :, here])

        @pl.when(block == z)
        def _():
            wide = cols // 2

            def one(i, carry):
                at = pl.ds(pl.multiple_of(i * wide, wide), wide)
                sh_part[:, at] = (dot_last(d_gate, s_g[at, :]) + dot_last(d_up, s_u[at, :])).astype(BF16)
                return carry

            lax.fori_loop(0, model // wide, one, 0)
            sh_copy.start()

    sh_copy = copy_to(sh_part.at[:, other], sh_in, misc_sem.at[0, 0], misc_sem.at[1, 0], me, 1 - core)

    def compute(block, way):
        for part in range(2):

            def one(d, carry):
                ref = lands[part].at[block, (q + width - d) % width, :, other]
                landed(ref, pair_sem.at[1, block, d, part])
                return carry

            lax.fori_loop(0, width, one, 0)

            def freed(d, carry):
                sent(ready.at[block, part, 0], plane_sem.at[0, block, d, part])
                return carry

            lax.fori_loop(1, width, freed, 0)
        inputs = land_t[block].reshape(slots, model)
        gate_pre = dot(inputs, w_g[...])
        up_pre = dot(inputs, w_u[...])
        active, slope = silu_parts(gate_pre)
        h = (active * up_pre).astype(BF16)
        h_cot = dot_last(land_c[block].reshape(slots, model), w_d[...])
        d_gate = (h_cot * up_pre * slope).astype(BF16)
        d_up = (h_cot * active).astype(BF16)
        hid[block] = h
        dgate[block] = d_gate
        dup[block] = d_up
        wide = cols // 2

        def half(which):
            def one(i, carry):
                at = pl.ds(pl.multiple_of(which * cols + i * wide, wide), wide)
                out = dot_last(d_gate, w_g[at, :]) + dot_last(d_up, w_u[at, :])
                here = pl.ds(pl.multiple_of(i * wide, wide), wide)
                ready[block, which, :, :, here] = out.astype(BF16).reshape(width, cap, wide)
                return carry

            lax.fori_loop(0, 2, one, 0)

        def one(i, carry):
            half((1 - core) * (1 - i) + core * i)

            @pl.when(i == 0)
            def _():
                tp_copy(block).start()

            return carry

        lax.fori_loop(0, 2, one, 0)
        gate_part[block] = row_sums(h.astype(F32) * h_cot)

    def sums(block, way):
        landed(tp_in.at[block], tp_sem.at[1, block])
        tp_in[block] = (ready[block, core].astype(F32) + tp_in[block].astype(F32)).astype(BF16)

        def one(d, carry):
            ret_copy(block, d).start()
            return carry

        lax.fori_loop(1, width, one, 0)
        ret_in[block, q] = tp_in[block, q]

    def scatter(block, way):
        def one(d, carry):
            landed(ret_in.at[block, q], ret_sem.at[1, block, d])
            return carry

        lax.fori_loop(1, width, one, 0)
        hit = jnp.where(hits(block), 1.0, 0.0).astype(BF16)
        back = dot_first(hit, ret_in[block].reshape(slots, cols))

        @pl.when(block == z)
        def _():
            routed[...] = back

        @pl.when(block != z)
        def _():
            z_out[block] = back.astype(BF16)
            z_copy(block).start()

    for part in range(2):
        loads[part].wait()
        for way in range(2):

            @pl.when(onward(way))
            def _():
                line_copy(way, z, part).start()

    acc_g[...] = jnp.zeros_like(acc_g)
    acc_u[...] = jnp.zeros_like(acc_u)
    acc_d[...] = jnp.zeros_like(acc_d)

    def body(step, carry):
        @pl.when(step == 1)
        def _():
            for load in loads[2:]:
                load.wait()
            for other_step in range(1, planes):
                landed(line_table.at[z], table_sem.at[1, other_step - 1])

        for part in range(2):

            def arrive(block, way):
                @pl.when(step > 0)
                def _():
                    landed(parts[part].at[block, :, mine], line_sem.at[1, way, block, part])

                    @pl.when(onward(way))
                    def _():
                        line_copy(way, block, part).start()

                    share_copy(block, part).start()

            each(step, arrive)
            each(step, lambda block, way: select(part, block))
        each(step - 1, shared)
        each(step - 1, pass_on)
        each(step - 1, compute)
        each(step - 1, sums)
        each(step - 2, scatter)
        return carry

    lax.fori_loop(0, planes + 1, body, 0)

    for p in range(width):
        at = slice(p * take, (p + 1) * take)
        deal_gu[p, 0] = acc_g[at, :].astype(BF16)
        deal_gu[p, 1] = acc_u[at, :].astype(BF16)
        deal_d[p] = acc_d[:, at].astype(BF16)

    def deal_copies(d):
        to_q = (q + d) % width
        peer = z * width + to_q
        return (
            copy_to(deal_gu.at[to_q], deal_gu_in.at[d], deal_sem.at[0, d, 0], deal_sem.at[1, d, 0], peer, core),
            copy_to(deal_d.at[to_q], deal_d_in.at[d], deal_sem.at[0, d, 1], deal_sem.at[1, d, 1], peer, core),
        )

    def deal(d, carry):
        for copy in deal_copies(d):
            copy.start()
        return carry

    lax.fori_loop(1, width, deal, 0)
    gate_pair = copy_to(gate_part, gate_in, misc_sem.at[0, 1], misc_sem.at[1, 1], me, 1 - core)
    gate_pair.start()
    gate_pair.wait_recv()
    gate_sum[...] = gate_part[...] + gate_in[...]
    gate_out[me] = gate_sum[z]

    def gate_copy(step):
        peer = (me + step) % experts
        return copy_to(
            gate_sum.at[peer // width], gate_out.at[me], gate_sem.at[0, step], gate_sem.at[1, step], peer, core
        )

    def send_gate(step, carry):
        gate_copy(step).start()
        return carry

    lax.fori_loop(1, experts, send_gate, 0)

    wide = stage_g.shape[1]
    chunks = model // wide

    def stage_copies(i, slot):
        at = pl.ds(pl.multiple_of(i * wide, wide), wide)
        return (
            pltpu.make_async_copy(stage_g.at[slot], gg_out.at[at, :], stage_sem.at[slot, 0]),
            pltpu.make_async_copy(stage_u.at[slot], gu_out.at[at, :], stage_sem.at[slot, 1]),
            pltpu.make_async_copy(stage_d.at[slot], gd_out.at[:, at], stage_sem.at[slot, 2]),
        )

    down_out[...] = jnp.zeros_like(down_out)
    norm_part[...] = jnp.zeros_like(norm_part)

    def weight_grads(i, carry):
        slot = i % 2
        at = pl.ds(pl.multiple_of(i * wide, wide), wide)

        @pl.when(i >= 2)
        def _():
            for copy in stage_copies(i - 2, slot):
                copy.wait()

        block_rows = land_t[:, :, :, at].reshape(planes * slots, wide)
        grad = dot_first(block_rows, dgate[...].reshape(planes * slots, hidden))
        stage_g[slot] = grad
        norm_part[0:1, at] = row_sums(grad * grad)
        grad = dot_first(block_rows, dup[...].reshape(planes * slots, hidden))
        stage_u[slot] = grad
        norm_part[1:2, at] = row_sums(grad * grad)
        block_rows = land_c[:, :, :, at].reshape(planes * slots, wide)
        grad = dot_first(hid[...].reshape(planes * slots, hidden), block_rows)
        stage_d[slot] = grad
        down_out[...] += row_sums(grad * grad)
        for copy in stage_copies(i, slot):
            copy.start()
        return carry

    lax.fori_loop(0, chunks, weight_grads, 0)
    each(planes - 1, scatter)

    def deal_done(d, carry):
        for copy in deal_copies(d):
            copy.wait_recv()
        return carry

    lax.fori_loop(1, width, deal_done, 0)
    grad_g, grad_u, grad_d = deal_gu[q, 0].astype(F32), deal_gu[q, 1].astype(F32), deal_d[q].astype(F32)
    for d in range(1, width):
        grad_g = grad_g + deal_gu_in[d, 0].astype(F32)
        grad_u = grad_u + deal_gu_in[d, 1].astype(F32)
        grad_d = grad_d + deal_d_in[d].astype(F32)
    sg_out[...] = grad_g
    su_out[...] = grad_u
    sd_out[...] = grad_d
    norm_part[2:3, :take] = row_sums(grad_g * grad_g)
    norm_part[3:4, :take] = row_sums(grad_u * grad_u)
    norm_pair = copy_to(norm_part, norm_in, misc_sem.at[0, 2], misc_sem.at[1, 2], me, 1 - core)
    norm_pair.start()
    sdn_part[...] = row_sums(grad_d * grad_d)
    sdn_out[me] = sdn_part[...]

    def sdn_copy(step):
        return copy_to(
            sdn_part, sdn_out.at[me], sdn_sem.at[0, step], sdn_sem.at[1, step], (me + step) % experts, core
        )

    def send_sdn(step, carry):
        sdn_copy(step).start()
        return carry

    lax.fori_loop(1, experts, send_sdn, 0)
    sh_copy.wait_recv()
    total = routed[...] + (sh_part[:, mine].astype(F32) + sh_in[...].astype(F32))
    routed[...] = total
    norm_pair.wait_recv()
    norm_out[...] = norm_part[...] + norm_in[...]

    def gather(step, carry):
        source = (z + step) % planes
        landed(z_in.at[source], z_sem.at[1, source])
        routed[...] += z_in[source].astype(F32)
        return carry

    lax.fori_loop(1, planes, gather, 0)
    tok_out[...] = routed[...].astype(BF16)

    def small_done(step, carry):
        gate_copy(step).wait()
        sdn_copy(step).wait()
        return carry

    lax.fori_loop(1, experts, small_done, 0)
    for i in range(max(chunks - 2, 0), chunks):
        for copy in stage_copies(i, i % 2):
            copy.wait()
    for step in range(1, planes):
        table_copy(step).wait_send()
    sh_copy.wait_send()
    gate_pair.wait_send()
    norm_pair.wait_send()

    def deal_sent(d, carry):
        for copy in deal_copies(d):
            copy.wait_send()
        return carry

    lax.fori_loop(1, width, deal_sent, 0)

    def drain(block, carry):
        for part in range(2):
            for way in range(2):
                behind = (block <= z) if way == 0 else (block >= z)

                @pl.when(behind & onward(way))
                def _():
                    line_copy(way, block, part).wait_send()

            @pl.when(block != z)
            def _():
                share_copy(block, part).wait_send()

            def pairs(d, inner):
                pair_copy(block, d, part).wait_send()
                return inner

            lax.fori_loop(0, width, pairs, 0)
        tp_copy(block).wait_send()

        def returns(d, inner):
            ret_copy(block, d).wait_send()
            return inner

        lax.fori_loop(1, width, returns, 0)

        @pl.when(block != z)
        def _():
            z_copy(block).wait_send()

        return carry

    lax.fori_loop(0, planes, drain, 0)


def layer(planes, cap, table, tokens, cotangent, w_gate, w_up, w_down, sh_gate, sh_up, sh_down):
    width = table.shape[2]
    experts = planes * width
    rows, model = tokens.shape
    cols, hidden = model // 2, w_gate.shape[1]
    take = model // experts
    span = width * take
    slots = width * cap
    wide = min(256, model)
    vmem = pl.BlockSpec(memory_space=pltpu.VMEM)
    hbm = pl.BlockSpec(memory_space=pltpu.HBM)
    out = jax.ShapeDtypeStruct
    dma = pltpu.SemaphoreType.DMA
    far = max(planes - 1, 1)
    return pl.pallas_call(
        functools.partial(layer_kernel, planes, width, cap),
        out_shape=(
            out((rows, cols), BF16),
            out((model, hidden), F32),
            out((model, hidden), F32),
            out((hidden, model), F32),
            out((take, hidden), F32),
            out((take, hidden), F32),
            out((hidden, take), F32),
            out((8, model), F32),
            out((1, hidden), F32),
            out((experts, 1, hidden), F32),
            out((experts, 1, slots), F32),
        ),
        in_specs=[vmem] + [hbm] * 8,
        out_specs=(vmem, hbm, hbm, hbm) + (vmem,) * 7,
        scratch_shapes=[
            pltpu.VMEM((planes, rows, model), BF16),
            pltpu.VMEM((planes, rows, model), BF16),
            pltpu.VMEM((planes,) + table.shape, F32),
            pltpu.VMEM((planes, 2, width, cap, cols), BF16),
            pltpu.VMEM((planes, width, cap, model), BF16),
            pltpu.VMEM((planes, width, cap, model), BF16),
            pltpu.VMEM((model, hidden), BF16),
            pltpu.VMEM((model, hidden), BF16),
            pltpu.VMEM((hidden, model), BF16),
            pltpu.VMEM((model, hidden), BF16),
            pltpu.VMEM((model, hidden), BF16),
            pltpu.VMEM((hidden, model), BF16),
            pltpu.VMEM((planes, slots, hidden), BF16),
            pltpu.VMEM((planes, slots, hidden), BF16),
            pltpu.VMEM((planes, slots, hidden), BF16),
            pltpu.VMEM((planes, width, cap, cols), BF16),
            pltpu.VMEM((planes, width, cap, cols), BF16),
            pltpu.VMEM((planes, rows, cols), BF16),
            pltpu.VMEM((planes, rows, cols), BF16),
            pltpu.VMEM((rows, cols), F32),
            pltpu.VMEM((2, wide, hidden), F32),
            pltpu.VMEM((2, wide, hidden), F32),
            pltpu.VMEM((2, hidden, wide), F32),
            pltpu.VMEM((span, hidden), F32),
            pltpu.VMEM((span, hidden), F32),
            pltpu.VMEM((hidden, span), F32),
            pltpu.VMEM((width, 2, take, hidden), BF16),
            pltpu.VMEM((width, hidden, take), BF16),
            pltpu.VMEM((width, 2, take, hidden), BF16),
            pltpu.VMEM((width, hidden, take), BF16),
            pltpu.VMEM((rows, model), BF16),
            pltpu.VMEM((rows, cols), BF16),
            pltpu.VMEM((planes, 1, slots), F32),
            pltpu.VMEM((planes, 1, slots), F32),
            pltpu.VMEM((planes, 1, slots), F32),
            pltpu.VMEM((8, model), F32),
            pltpu.VMEM((8, model), F32),
            pltpu.VMEM((1, hidden), F32),
            dma((8,)),
            dma((2, far)),
            dma((2, 2, planes, 2)),
            dma((2, planes, 2)),
            dma((2, planes, width, 2)),
            dma((2, planes, width, 2)),
            dma((2, planes)),
            dma((2, planes, width)),
            dma((2, planes)),
            dma((2, width, 2)),
            dma((2, 3)),
            dma((2, experts)),
            dma((2, experts)),
            dma((2, 3)),
        ],
        compiler_params=pltpu.CompilerParams(has_side_effects=True, vmem_limit_bytes=67043328),
        name="layer",
    )(table, tokens, cotangent, w_gate, w_up, w_down, sh_gate, sh_up, sh_down)


def local(planes, tokens, expert_ids, gates, cotangent, w_gate, w_up, w_down, sh_gate, sh_up, sh_down):
    experts = lax.axis_size("ep")
    width = experts // planes
    q = lax.axis_index("ep") % width
    rows, model = tokens.shape
    top_count = expert_ids.shape[1]
    capacity = 3 * rows * top_count // (2 * experts)

    lanes = jnp.arange(experts, dtype=jnp.int32)
    earlier = jnp.tril(jnp.ones((rows, rows), BF16), -1)
    mine = expert_ids[:, :, None] == lanes
    names = jnp.any(mine, axis=1)
    rank = jnp.dot(earlier, names.astype(BF16), preferred_element_type=F32)
    rank = jnp.where(names, rank.astype(jnp.int32), -1)
    gate_of = jnp.sum(jnp.where(mine, gates[:, :, None], 0.0), axis=1)
    table = jnp.stack([rank.T.astype(F32), gate_of.T]).reshape(2, planes, width, 1, rows)
    cap = -(-capacity // 8) * 8
    (token_grad, grad_g, grad_u, grad_d, out_g, out_u, out_d, norms, down, shared_down, gate_rows) = layer(
        planes, cap, table, tokens, cotangent, w_gate[0], w_up[0], w_down[0], sh_gate, sh_up, sh_down
    )
    back_gate = lax.dynamic_slice_in_dim(gate_rows.reshape(experts, width, cap), q, 1, 1)[:, 0]
    slots = jnp.arange(cap, dtype=jnp.int32)
    picked = rank.T[:, None, :] == slots[None, :, None]
    token_gate = jnp.sum(jnp.where(picked, back_gate[:, :, None], 0.0), axis=1)
    gate_grad = jnp.sum(jnp.where(mine, token_gate.T[:, None, :], 0.0), axis=2) / gates
    take = model // experts
    return (
        token_grad,
        gate_grad,
        grad_g[None],
        grad_u[None],
        grad_d[None],
        out_g,
        out_u,
        out_d,
        norms[0:1],
        norms[1:2],
        down,
        norms[2, :take],
        norms[3, :take],
        jnp.sum(shared_down[:, 0], axis=0),
    )


def solution(mesh):
    placed = (
        P("ep", None),
        P("ep", None),
        P("ep", None),
        P("ep", None),
        P("ep", None, "tp"),
        P("ep", None, "tp"),
        P("ep", "tp", None),
        P(None, "tp"),
        P(None, "tp"),
        P("tp", None),
    )
    return jax.shard_map(
        functools.partial(local, plane_count(mesh)),
        mesh=mesh,
        in_specs=placed,
        out_specs=(
            P("ep", "tp"),
            P("ep", None),
            P("ep", None, "tp"),
            P("ep", None, "tp"),
            P("ep", "tp", None),
            P("ep", "tp"),
            P("ep", "tp"),
            P("tp", "ep"),
            P("ep", None),
            P("ep", None),
            P("ep", "tp"),
            P("ep"),
            P("ep"),
            P("tp"),
        ),
        check_vma=False,
    )
```

```python
import functools
import math

import jax
import jax.numpy as jnp
from jax import lax
from jax.experimental import pallas as pl
from jax.experimental.pallas import tpu as pltpu
from jax.sharding import PartitionSpec as P

BF16 = jnp.bfloat16
F32 = jnp.float32
LAST = (((1,), (1,)), ((), ()))
FIRST = (((0,), (0,)), ((), ()))


def silu_parts(pre):
    sigmoid = jax.nn.sigmoid(pre)
    return (pre * sigmoid, sigmoid * (1.0 + pre * (1.0 - sigmoid)))


def dot(left, right):
    return jnp.dot(left, right, preferred_element_type=F32)


def dot_last(left, right):
    return lax.dot_general(left, right, LAST, preferred_element_type=F32)


def dot_first(left, right):
    return lax.dot_general(left, right, FIRST, preferred_element_type=F32)


def row_sums(values):
    ones = jnp.ones((8, values.shape[1]), F32)
    sums = lax.dot_general(
        ones, values, LAST, precision=lax.Precision.HIGHEST, preferred_element_type=F32
    )
    return sums[:1]


def plane_count(mesh):
    count = mesh.shape["ep"]
    try:
        planes = len({tuple(d.coords)[2] for d in mesh.devices.flat})
    except (AttributeError, TypeError, IndexError):
        planes = 0
    if planes < 1 or count % planes:
        planes = max(d for d in range(1, math.isqrt(count) + 1) if count % d == 0)
    return planes


def copy_to(src, dst, send, recv, ep, tp):
    return pltpu.make_async_remote_copy(
        src_ref=src,
        dst_ref=dst,
        send_sem=send,
        recv_sem=recv,
        device_id=(ep, tp),
        device_id_type=pl.DeviceIdType.MESH,
    )


def layer_kernel(
    planes, width, cap,
    ids, gates, tokens, cotangent, wg_in, wu_in, wd_in, sg_in, su_in, sd_in,
    tok_out, gate_out, gg_out, gu_out, gd_out, sg_out, su_out, sd_out,
    gn_out, un_out, dn_out, sgn_out, sun_out, sdn_out,
    toks, cots, own_table, line_table, ready, land_t, land_c,
    w_g, w_u, w_d, s_g, s_u, s_d,
    hid, dgate, dup, act, slant, tp_in, ret_in, z_out, z_in, routed,
    stage_g, stage_u, stage_d, acc_g, acc_u, acc_d,
    deal_gu, deal_d, deal_gu_in, deal_d_in, sh_part, sh_in,
    gate_part, gate_in, gate_sum, gate_back, norm_part, norm_in, sdn_part, sdn_in,
    tok_done, gate_done, sg_done, su_done, sd_done, gn_done, un_done, dn_done, sgn_done, sun_done, sdn_done,
    load_sem, table_sem, line_sem, share_sem, plane_sem, pair_sem, tp_sem, ret_sem, z_sem,
    deal_sem, misc_sem, pair_gate_sem, gate_sem, sdn_sem, stage_sem, out_sem,
):
    me, core = lax.axis_index("ep"), lax.axis_index("tp")
    z, q = me // width, me % width
    experts = planes * width
    rows, model = tokens.shape
    cols = model // 2
    hidden = w_g.shape[1]
    slots = width * cap
    take = model // experts
    span = width * take
    mine = pl.ds(pl.multiple_of(core * cols, cols), cols)
    other = pl.ds(pl.multiple_of((1 - core) * cols, cols), cols)
    parts = (toks, cots)
    lands = (land_t, land_c)

    def landed(ref, sem):
        copy_to(ref, ref, sem, sem, me, 1 - core).wait_recv()

    def sent(ref, sem):
        copy_to(ref, ref, sem, sem, me, 1 - core).wait_send()

    loads = [
        pltpu.make_async_copy(src, dst, load_sem.at[i])
        for i, (src, dst) in enumerate(
            (
                (tokens, toks.at[z]),
                (cotangent, cots.at[z]),
                (sg_in, s_g),
                (su_in, s_u),
                (sd_in, s_d),
                (wg_in, w_g),
                (wu_in, w_u),
                (wd_in, w_d),
            )
        )
    ]
    for load in loads[:2]:
        load.start()
    flushed = []
    barrier = pltpu.get_barrier_semaphore()

    def greet(ep, tp):
        pl.semaphore_signal(
            barrier, inc=1, device_id=(ep, tp), device_id_type=pl.DeviceIdType.MESH
        )

    def greet_peer(step, carry):
        greet((me + step) % experts, core)
        return carry

    greet(me, 1 - core)
    lax.fori_loop(1, experts, greet_peer, 0)

    def flush(src, dst):
        copy = pltpu.make_async_copy(src, dst, out_sem.at[len(flushed)])
        copy.start()
        flushed.append(copy)

    def onward(way):
        there = z + 1 - 2 * way
        return (there >= 0) & (there < planes)

    def line_copy(way, block, part, source=None):
        there = jnp.clip(z + 1 - 2 * way, 0, planes - 1)
        ref = parts[part].at[block, :, mine]
        return copy_to(
            ref if source is None else source,
            ref,
            line_sem.at[0, way, block, part],
            line_sem.at[1, way, block, part],
            there * width + q,
            core,
        )

    def line_start(part, source):
        for way in range(2):

            @pl.when(onward(way))
            def _():
                line_copy(way, z, part, source.at[:, mine]).start()

    named = lax.broadcasted_iota(jnp.int32, (experts, rows), 0)
    names, gate_of = jnp.zeros((experts, rows), F32), jnp.zeros((experts, rows), F32)
    for k in range(ids.shape[0]):
        same = named == ids[k : k + 1, :]
        names = names + jnp.where(same, 1.0, 0.0)
        gate_of = gate_of + jnp.where(same, gates[k : k + 1, :], 0.0)
    before = lax.broadcasted_iota(jnp.int32, (rows, rows), 0) < lax.broadcasted_iota(jnp.int32, (rows, rows), 1)
    rank = dot(names.astype(BF16), jnp.where(before, 1.0, 0.0).astype(BF16))
    rank = jnp.where(names > 0.0, rank, -1.0)
    for e in range(experts):
        own_table[e // width, 0, e % width] = rank[e : e + 1, :]
        own_table[e // width, 1, e % width] = gate_of[e : e + 1, :]
    line_table[z] = own_table[z]
    pl.semaphore_wait(barrier, experts)
    line_start(0, tokens)

    def table_copy(step):
        there = (z + step) % planes
        return copy_to(
            own_table.at[there], line_table.at[z], table_sem.at[0, step - 1], table_sem.at[1, step - 1],
            there * width + q, core,
        )

    for step in range(1, planes):
        table_copy(step).start()
    line_start(1, cotangent)

    def share_copy(block, part):
        ref = parts[part].at[block, :, mine]
        return copy_to(ref, ref, share_sem.at[0, block, part], share_sem.at[1, block, part], me, 1 - core)

    def plane_copy(block, d, part):
        to_q = (q + d) % width
        return copy_to(
            ready.at[block, part, to_q],
            lands[part].at[block, q, :, mine],
            plane_sem.at[0, block, d, part],
            plane_sem.at[1, block, d, part],
            z * width + to_q,
            core,
        )

    def pair_copy(block, d, part):
        ref = lands[part].at[block, (q + width - d) % width, :, mine]
        return copy_to(
            ref, ref, pair_sem.at[0, block, d, part], pair_sem.at[1, block, d, part], me, 1 - core
        )

    def tp_copy(block):
        return copy_to(
            ready.at[block, 1 - core], tp_in.at[block], tp_sem.at[0, block], tp_sem.at[1, block],
            me, 1 - core,
        )

    def ret_copy(block, d):
        to_q = (q + d) % width
        return copy_to(
            tp_in.at[block, to_q], ret_in.at[block, q], ret_sem.at[0, block, d], ret_sem.at[1, block, d],
            z * width + to_q, core,
        )

    def z_copy(block):
        return copy_to(
            z_out.at[block], z_in.at[z], z_sem.at[0, block], z_sem.at[1, z], block * width + q, core
        )

    def hits(block):
        ranks = line_table[block, 0]
        at = lax.broadcasted_iota(jnp.int32, (width, cap, rows), 1).astype(F32)
        return (at == ranks).reshape(slots, rows)

    inner = jnp.where(2 * z <= planes - 1, 1, 0)

    def each(step, act, ranks=(0, 2)):
        def one(rank, carry):
            way = inner + rank - 2 * inner * rank
            block = z - step + 2 * step * way
            valid = (step >= 0) & (block >= 0) & (block < planes) & ((step > 0) | (rank == 0))

            @pl.when(valid)
            def _():
                act(jnp.clip(block, 0, planes - 1), way)

            return carry

        lax.fori_loop(*ranks, one, 0)

    def select(part, block):
        hit = hits(block)
        picked = dot(jnp.where(hit, 1.0, 0.0).astype(BF16), parts[part][block, :, mine])
        if part == 1:
            gate_of = jnp.broadcast_to(line_table[block, 1], (width, cap, rows)).reshape(slots, rows)
            picked = picked * jnp.sum(jnp.where(hit, gate_of, 0.0), axis=1, keepdims=True)
        ready[block, part] = picked.astype(BF16).reshape(width, cap, cols)

        def one(d, carry):
            plane_copy(block, d, part).start()
            return carry

        lax.fori_loop(1, width, one, 0)
        lands[part][block, q, :, mine] = ready[block, part, q]
        pair_copy(block, 0, part).start()

    def pass_on(part, block):
        def one(d, carry):
            landed(lands[part].at[block, q, :, mine], plane_sem.at[1, block, d, part])
            pair_copy(block, d, part).start()
            return carry

        lax.fori_loop(1, width, one, 0)

    def paired(part, block):
        def one(d, carry):
            landed(lands[part].at[block, (q + width - d) % width, :, other], pair_sem.at[1, block, d, part])
            return carry

        lax.fori_loop(0, width, one, 0)

        def freed(d, carry):
            sent(ready.at[block, part, 0], plane_sem.at[0, block, d, part])
            return carry

        lax.fori_loop(1, width, freed, 0)

    def shared(block, way):
        for part in range(2):

            @pl.when(block != z)
            def _():
                landed(parts[part].at[block, :, other], share_sem.at[1, block, part])

        gate_pre = dot(toks[block], s_g[...])
        up_pre = dot(toks[block], s_u[...])
        active, slope = silu_parts(gate_pre)
        h = (active * up_pre).astype(BF16)
        h_cot = dot_last(cots[block], s_d[...])
        d_gate = (h_cot * up_pre * slope).astype(BF16)
        d_up = (h_cot * active).astype(BF16)
        here = pl.ds(pl.multiple_of(z * span, span), span)
        acc_g[...] += dot_first(toks[block, :, here], d_gate)
        acc_u[...] += dot_first(toks[block, :, here], d_up)
        acc_d[...] += dot_first(h, cots[block, :, here])

        @pl.when(block == z)
        def _():
            wide = cols // 2

            def one(i, carry):
                at = pl.ds(pl.multiple_of(i * wide, wide), wide)
                sh_part[:, at] = (dot_last(d_gate, s_g[at, :]) + dot_last(d_up, s_u[at, :])).astype(BF16)
                return carry

            lax.fori_loop(0, model // wide, one, 0)
            sh_copy.start()

    sh_copy = copy_to(sh_part.at[:, other], sh_in, misc_sem.at[0, 0], misc_sem.at[1, 0], me, 1 - core)

    def compute(last, block):
        paired(0, block)
        inputs = land_t[block].reshape(slots, model)
        gate_pre = dot(inputs, w_g[...])
        up_pre = dot(inputs, w_u[...])
        active, slope = silu_parts(gate_pre)
        act[...] = active
        slant[...] = up_pre * slope
        hid[block] = (active * up_pre).astype(BF16)

        @pl.when(last)
        def _():
            pass_on(1, block)

        paired(1, block)
        h_cot = dot_last(land_c[block].reshape(slots, model), w_d[...])
        d_gate = (h_cot * slant[...]).astype(BF16)
        d_up = (h_cot * act[...]).astype(BF16)
        dgate[block] = d_gate
        dup[block] = d_up
        gate_row = row_sums(hid[block].astype(F32) * h_cot)
        for w in range(width):
            gate_part[block, w, :, :cap] = gate_row[:, w * cap : (w + 1) * cap]
        gate_pair(block).start()
        wide = cols // 2

        def half(which):
            def one(i, carry):
                at = pl.ds(pl.multiple_of(which * cols + i * wide, wide), wide)
                out = dot_last(d_gate, w_g[at, :]) + dot_last(d_up, w_u[at, :])
                here = pl.ds(pl.multiple_of(i * wide, wide), wide)
                ready[block, which, :, :, here] = out.astype(BF16).reshape(width, cap, wide)
                return carry

            lax.fori_loop(0, 2, one, 0)

        def one(i, carry):
            half((1 - core) * (1 - i) + core * i)

            @pl.when(i == 0)
            def _():
                tp_copy(block).start()

            return carry

        lax.fori_loop(0, 2, one, 0)

    def gate_pair(block):
        return copy_to(
            gate_part.at[block], gate_in.at[block], pair_gate_sem.at[0, block], pair_gate_sem.at[1, block],
            me, 1 - core,
        )

    def gate_copy(block, d):
        to_q = (q + d) % width
        return copy_to(
            gate_sum.at[block, to_q], gate_back.at[me], gate_sem.at[0, block, d], gate_sem.at[1, z, d],
            block * width + to_q, core,
        )

    def gate_sends(block, way):
        gate_pair(block).wait_recv()
        gate_sum[block] = gate_part[block] + gate_in[block]

        def one(d, carry):
            @pl.when((block != z) | (d > 0))
            def _():
                gate_copy(block, d).start()

            return carry

        lax.fori_loop(0, width, one, 0)

        @pl.when(block == z)
        def _():
            gate_back[me] = gate_sum[z, q]

    def sums(block, way):
        landed(tp_in.at[block], tp_sem.at[1, block])
        tp_in[block] = (ready[block, core].astype(F32) + tp_in[block].astype(F32)).astype(BF16)

        def one(d, carry):
            ret_copy(block, d).start()
            return carry

        lax.fori_loop(1, width, one, 0)
        ret_in[block, q] = tp_in[block, q]

    def scatter(block, way):
        def one(d, carry):
            landed(ret_in.at[block, q], ret_sem.at[1, block, d])
            return carry

        lax.fori_loop(1, width, one, 0)
        hit = jnp.where(hits(block), 1.0, 0.0).astype(BF16)
        back = dot_first(hit, ret_in[block].reshape(slots, cols))

        @pl.when(block == z)
        def _():
            routed[...] = back

        @pl.when(block != z)
        def _():
            z_out[block] = back.astype(BF16)
            z_copy(block).start()

    for load in loads[:2]:
        load.wait()
    for load in loads[2:]:
        load.start()
    acc_g[...] = jnp.zeros_like(acc_g)
    acc_u[...] = jnp.zeros_like(acc_u)
    acc_d[...] = jnp.zeros_like(acc_d)
    gate_part[...] = jnp.zeros_like(gate_part)

    def body(step, carry):
        @pl.when(step == 1)
        def _():
            for load in loads[2:]:
                load.wait()
            for other_step in range(1, planes):
                landed(line_table.at[z], table_sem.at[1, other_step - 1])

        def expert(last, block):
            compute(last, block)

            @pl.when(block != z)
            def _():
                sums(block, 0)

            gate_sends(block, 0)

        def ahead(block, way):
            pass_on(0, block)
            pass_on(1, block)
            expert(False, block)

        early = (step == 2) & between

        @pl.when(early)
        def _():
            each(1, ahead, (0, 1))

        for part in range(2):

            def arrive(block, way):
                @pl.when(step > 0)
                def _():
                    landed(parts[part].at[block, :, mine], line_sem.at[1, way, block, part])

                    @pl.when(onward(way))
                    def _():
                        line_copy(way, block, part).start()

                    share_copy(block, part).start()

            each(step, arrive)
            each(step, lambda block, way: select(part, block), (0, 1))

        def select_both(block, way):
            for part in range(2):
                select(part, block)

        each(step, select_both, (1, 2))
        last = step == planes
        start = jnp.where(early, 1, 0)

        @pl.when((step > 2) & (step < planes))
        def _():
            each(step - 2, scatter, (0, 1))

        def hand_on(block, way):
            pass_on(0, block)

            @pl.when(jnp.logical_not(last))
            def _():
                pass_on(1, block)

        each(step - 1, hand_on, (start, 2))
        each(step - 1, shared)

        each(step - 1, lambda block, way: expert(last, block), (start, 2))

        @pl.when(step > 2)
        def _():
            each(step - 2, scatter, (jnp.where(last, 0, 1), 2))

        return carry

    between = (z > 0) & (z < planes - 1)
    lax.fori_loop(0, planes + 1, body, 0)

    for p in range(width):
        at = slice(p * take, (p + 1) * take)
        deal_gu[p, 0] = acc_g[at, :].astype(BF16)
        deal_gu[p, 1] = acc_u[at, :].astype(BF16)
        deal_d[p] = acc_d[:, at].astype(BF16)

    def deal_copies(d):
        to_q = (q + d) % width
        peer = z * width + to_q
        return (
            copy_to(deal_gu.at[to_q], deal_gu_in.at[d], deal_sem.at[0, d, 0], deal_sem.at[1, d, 0], peer, core),
            copy_to(deal_d.at[to_q], deal_d_in.at[d], deal_sem.at[0, d, 1], deal_sem.at[1, d, 1], peer, core),
        )

    def deal(d, carry):
        for copy in deal_copies(d):
            copy.start()
        return carry

    lax.fori_loop(1, width, deal, 0)
    sums(z, 0)
    wide = stage_g.shape[1]
    chunks = model // wide

    def stage_copies(i, slot):
        at = pl.ds(pl.multiple_of(i * wide, wide), wide)
        return (
            pltpu.make_async_copy(stage_g.at[slot], gg_out.at[at, :], stage_sem.at[slot, 0]),
            pltpu.make_async_copy(stage_u.at[slot], gu_out.at[at, :], stage_sem.at[slot, 1]),
            pltpu.make_async_copy(stage_d.at[slot], gd_out.at[:, at], stage_sem.at[slot, 2]),
        )

    dn_done[...] = jnp.zeros_like(dn_done)
    norm_part[...] = jnp.zeros_like(norm_part)

    def weight_grads(i, carry):
        slot = i % 2
        at = pl.ds(pl.multiple_of(i * wide, wide), wide)

        @pl.when(i >= 2)
        def _():
            for copy in stage_copies(i - 2, slot):
                copy.wait()

        block_rows = land_t[:, :, :, at].reshape(planes * slots, wide)
        grad = dot_first(block_rows, dgate[...].reshape(planes * slots, hidden))
        stage_g[slot] = grad
        norm_part[0:1, at] = row_sums(grad * grad)
        grad = dot_first(block_rows, dup[...].reshape(planes * slots, hidden))
        stage_u[slot] = grad
        norm_part[1:2, at] = row_sums(grad * grad)
        block_rows = land_c[:, :, :, at].reshape(planes * slots, wide)
        grad = dot_first(hid[...].reshape(planes * slots, hidden), block_rows)
        stage_d[slot] = grad
        dn_done[...] += row_sums(grad * grad)
        for copy in stage_copies(i, slot):
            copy.start()

        @pl.when(i == chunks // 4)
        def _():
            each(planes - 1, scatter)

        return carry

    lax.fori_loop(0, chunks, weight_grads, 0)
    flush(dn_done, dn_out)

    def deal_done(d, carry):
        for copy in deal_copies(d):
            copy.wait_recv()
        return carry

    lax.fori_loop(1, width, deal_done, 0)
    grad_g, grad_u, grad_d = deal_gu[q, 0].astype(F32), deal_gu[q, 1].astype(F32), deal_d[q].astype(F32)
    for d in range(1, width):
        grad_g = grad_g + deal_gu_in[d, 0].astype(F32)
        grad_u = grad_u + deal_gu_in[d, 1].astype(F32)
        grad_d = grad_d + deal_d_in[d].astype(F32)
    sg_done[...] = grad_g
    su_done[...] = grad_u
    sd_done[...] = grad_d
    flush(sg_done, sg_out)
    flush(su_done, su_out)
    flush(sd_done, sd_out)
    norm_part[2:3, :take] = row_sums(grad_g * grad_g)
    norm_part[3:4, :take] = row_sums(grad_u * grad_u)
    norm_pair = copy_to(norm_part, norm_in, misc_sem.at[0, 2], misc_sem.at[1, 2], me, 1 - core)
    norm_pair.start()
    sdn_part[...] = row_sums(grad_d * grad_d)
    sdn_in[me] = sdn_part[...]

    def sdn_copy(step):
        return copy_to(
            sdn_part, sdn_in.at[me], sdn_sem.at[0, step], sdn_sem.at[1, step], (me + step) % experts, core
        )

    def send_sdn(step, carry):
        sdn_copy(step).start()
        return carry

    lax.fori_loop(1, experts, send_sdn, 0)
    norm_pair.wait_recv()
    total = norm_part[...] + norm_in[...]
    gn_done[...] = total[0:1]
    un_done[...] = total[1:2]
    sgn_done[...] = total[2:3, :take]
    sun_done[...] = total[3:4, :take]
    flush(gn_done, gn_out)
    flush(un_done, un_out)
    flush(sgn_done, sgn_out)
    flush(sun_done, sun_out)

    def gate_arrived(source, carry):
        def one(d, inner):
            @pl.when((source != z) | (d > 0))
            def _():
                landed(gate_back.at[me], gate_sem.at[1, source, d])

            return inner

        return lax.fori_loop(0, width, one, carry)

    lax.fori_loop(0, planes, gate_arrived, 0)
    top, lanes = ids.shape[0], gate_back.shape[2]

    def gate_rows(e, total):
        at = lax.broadcasted_iota(jnp.int32, (lanes, rows), 0).astype(F32)
        hit = jnp.where(at == own_table[e // width, 0, e % width], 1.0, 0.0)
        back = lax.dot_general(
            jnp.broadcast_to(gate_back[e], (8, lanes)), hit, (((1,), (0,)), ((), ())),
            precision=lax.Precision.HIGHEST, preferred_element_type=F32,
        )
        return total + jnp.where(ids[...] == e, jnp.broadcast_to(back[:1], (top, rows)), 0.0)

    total = lax.fori_loop(0, experts, gate_rows, jnp.zeros((top, rows), F32))
    gate_done[...] = total / gates[...]
    flush(gate_done, gate_out)

    scatter(z, 0)
    sh_copy.wait_recv()
    routed[...] += sh_part[:, mine].astype(F32) + sh_in[...].astype(F32)

    def gather(step, carry):
        source = (z + step) % planes
        landed(z_in.at[source], z_sem.at[1, source])
        routed[...] += z_in[source].astype(F32)
        return carry

    lax.fori_loop(1, planes, gather, 0)
    tok_done[...] = routed[...].astype(BF16)
    flush(tok_done, tok_out)

    def small_done(step, carry):
        sdn_copy(step).wait()
        return carry

    lax.fori_loop(1, experts, small_done, 0)
    sdn_done[...] = jnp.sum(sdn_in[...], axis=0)
    flush(sdn_done, sdn_out)
    for i in range(max(chunks - 2, 0), chunks):
        for copy in stage_copies(i, i % 2):
            copy.wait()
    for step in range(1, planes):
        table_copy(step).wait_send()
    sh_copy.wait_send()
    norm_pair.wait_send()

    def deal_sent(d, carry):
        for copy in deal_copies(d):
            copy.wait_send()
        return carry

    lax.fori_loop(1, width, deal_sent, 0)

    def drain(block, carry):
        for part in range(2):
            for way in range(2):
                behind = (block <= z) if way == 0 else (block >= z)

                @pl.when(behind & onward(way))
                def _():
                    sent(parts[part].at[block, :, mine], line_sem.at[0, way, block, part])

            @pl.when(block != z)
            def _():
                share_copy(block, part).wait_send()

            def pairs(d, inner):
                pair_copy(block, d, part).wait_send()
                return inner

            lax.fori_loop(0, width, pairs, 0)
        tp_copy(block).wait_send()
        gate_pair(block).wait_send()

        def gate_sent(d, inner):
            @pl.when((block != z) | (d > 0))
            def _():
                gate_copy(block, d).wait_send()

            return inner

        lax.fori_loop(0, width, gate_sent, 0)

        def returns(d, inner):
            ret_copy(block, d).wait_send()
            return inner

        lax.fori_loop(1, width, returns, 0)

        @pl.when(block != z)
        def _():
            z_copy(block).wait_send()

        return carry

    lax.fori_loop(0, planes, drain, 0)
    for copy in flushed:
        copy.wait()


def finish_kernel(count, *refs):
    sources, results, held = refs[:count], refs[count : 2 * count], refs[2 * count : 3 * count]
    in_sem, out_sem = refs[3 * count :]
    moves = []
    for i in range(count):
        rows = sources[i].shape[0]
        pieces = 4 if rows % 32 == 0 and sources[i].shape[1] * rows >= 2**18 else 1
        step = rows // pieces
        for p in range(pieces):
            at = slice(p * step, (p + 1) * step)
            moves.append(
                (
                    pltpu.make_async_copy(sources[i].at[at], held[i].at[at], in_sem.at[i, p]),
                    pltpu.make_async_copy(held[i].at[at], results[i].at[at], out_sem.at[i, p]),
                )
            )
    for taken, _ in moves:
        taken.start()
    for taken, given in moves:
        taken.wait()
        given.start()
    for _, given in moves:
        given.wait()


def finish(arrays):
    count = len(arrays)
    hbm = pl.BlockSpec(memory_space=pltpu.HBM)
    return pl.pallas_call(
        functools.partial(finish_kernel, count),
        out_shape=[jax.ShapeDtypeStruct(a.shape, a.dtype) for a in arrays],
        in_specs=[hbm] * count,
        out_specs=[hbm] * count,
        scratch_shapes=[pltpu.VMEM(a.shape, a.dtype) for a in arrays]
        + [pltpu.SemaphoreType.DMA((count, 4)), pltpu.SemaphoreType.DMA((count, 4))],
        compiler_params=pltpu.CompilerParams(vmem_limit_bytes=67043328),
        name="finish",
    )(*arrays)


def layer(planes, cap, ids, gates, tokens, cotangent, w_gate, w_up, w_down, sh_gate, sh_up, sh_down):
    experts = lax.axis_size("ep")
    width = experts // planes
    rows, model = tokens.shape
    lanes = -(-cap // 128) * 128
    cols, hidden = model // 2, w_gate.shape[1]
    take = model // experts
    span = width * take
    slots = width * cap
    wide = min(256, model)
    vmem = pl.BlockSpec(memory_space=pltpu.VMEM)
    hbm = pl.BlockSpec(memory_space=pltpu.HBM)
    out = jax.ShapeDtypeStruct
    dma = pltpu.SemaphoreType.DMA
    far = max(planes - 1, 1)
    return pl.pallas_call(
        functools.partial(layer_kernel, planes, width, cap),
        out_shape=(
            out((rows, cols), BF16),
            out(gates.shape, F32),
            out((model, hidden), F32),
            out((model, hidden), F32),
            out((hidden, model), F32),
            out((take, hidden), F32),
            out((take, hidden), F32),
            out((hidden, take), F32),
            out((1, model), F32),
            out((1, model), F32),
            out((1, hidden), F32),
            out((1, take), F32),
            out((1, take), F32),
            out((1, hidden), F32),
        ),
        in_specs=[vmem] * 2 + [hbm] * 8,
        out_specs=(hbm,) * 14,
        scratch_shapes=[
            pltpu.VMEM((planes, rows, model), BF16),
            pltpu.VMEM((planes, rows, model), BF16),
            pltpu.VMEM((planes, 2, width, 1, rows), F32),
            pltpu.VMEM((planes, 2, width, 1, rows), F32),
            pltpu.VMEM((planes, 2, width, cap, cols), BF16),
            pltpu.VMEM((planes, width, cap, model), BF16),
            pltpu.VMEM((planes, width, cap, model), BF16),
            pltpu.VMEM((model, hidden), BF16),
            pltpu.VMEM((model, hidden), BF16),
            pltpu.VMEM((hidden, model), BF16),
            pltpu.VMEM((model, hidden), BF16),
            pltpu.VMEM((model, hidden), BF16),
            pltpu.VMEM((hidden, model), BF16),
            pltpu.VMEM((planes, slots, hidden), BF16),
            pltpu.VMEM((planes, slots, hidden), BF16),
            pltpu.VMEM((planes, slots, hidden), BF16),
            pltpu.VMEM((slots, hidden), F32),
            pltpu.VMEM((slots, hidden), F32),
            pltpu.VMEM((planes, width, cap, cols), BF16),
            pltpu.VMEM((planes, width, cap, cols), BF16),
            pltpu.VMEM((planes, rows, cols), BF16),
            pltpu.VMEM((planes, rows, cols), BF16),
            pltpu.VMEM((rows, cols), F32),
            pltpu.VMEM((2, wide, hidden), F32),
            pltpu.VMEM((2, wide, hidden), F32),
            pltpu.VMEM((2, hidden, wide), F32),
            pltpu.VMEM((span, hidden), F32),
            pltpu.VMEM((span, hidden), F32),
            pltpu.VMEM((hidden, span), F32),
            pltpu.VMEM((width, 2, take, hidden), BF16),
            pltpu.VMEM((width, hidden, take), BF16),
            pltpu.VMEM((width, 2, take, hidden), BF16),
            pltpu.VMEM((width, hidden, take), BF16),
            pltpu.VMEM((rows, model), BF16),
            pltpu.VMEM((rows, cols), BF16),
            pltpu.VMEM((planes, width, 1, lanes), F32),
            pltpu.VMEM((planes, width, 1, lanes), F32),
            pltpu.VMEM((planes, width, 1, lanes), F32),
            pltpu.VMEM((experts, 1, lanes), F32),
            pltpu.VMEM((8, model), F32),
            pltpu.VMEM((8, model), F32),
            pltpu.VMEM((1, hidden), F32),
            pltpu.VMEM((experts, 1, hidden), F32),
            pltpu.VMEM((rows, cols), BF16),
            pltpu.VMEM(gates.shape, F32),
            pltpu.VMEM((take, hidden), F32),
            pltpu.VMEM((take, hidden), F32),
            pltpu.VMEM((hidden, take), F32),
            pltpu.VMEM((1, model), F32),
            pltpu.VMEM((1, model), F32),
            pltpu.VMEM((1, hidden), F32),
            pltpu.VMEM((1, take), F32),
            pltpu.VMEM((1, take), F32),
            pltpu.VMEM((1, hidden), F32),
            dma((8,)),
            dma((2, far)),
            dma((2, 2, planes, 2)),
            dma((2, planes, 2)),
            dma((2, planes, width, 2)),
            dma((2, planes, width, 2)),
            dma((2, planes)),
            dma((2, planes, width)),
            dma((2, planes)),
            dma((2, width, 2)),
            dma((2, 3)),
            dma((2, planes)),
            dma((2, planes, width)),
            dma((2, experts)),
            dma((2, 3)),
            dma((16,)),
        ],
        compiler_params=pltpu.CompilerParams(collective_id=0, has_side_effects=True, vmem_limit_bytes=67043328),
        name="layer",
    )(ids, gates, tokens, cotangent, w_gate, w_up, w_down, sh_gate, sh_up, sh_down)


def local(planes, tokens, expert_ids, gates, cotangent, w_gate, w_up, w_down, sh_gate, sh_up, sh_down):
    experts = lax.axis_size("ep")
    rows, top_count = expert_ids.shape
    capacity = 3 * rows * top_count // (2 * experts)
    cap = -(-capacity // 8) * 8
    arrays = layer(
        planes, cap, expert_ids.T, gates.T, tokens, cotangent,
        w_gate[0], w_up[0], w_down[0], sh_gate, sh_up, sh_down,
    )
    (token_grad, gate_grad, grad_g, grad_u, grad_d, out_g, out_u, out_d, gate_norms, up_norms, down_norms,
     shared_gate, shared_up, shared_down) = finish(arrays)
    return (
        token_grad,
        gate_grad.T,
        grad_g[None],
        grad_u[None],
        grad_d[None],
        out_g,
        out_u,
        out_d,
        gate_norms,
        up_norms,
        down_norms,
        shared_gate[0],
        shared_up[0],
        shared_down[0],
    )


def solution(mesh):
    placed = (
        P("ep", None),
        P("ep", None),
        P("ep", None),
        P("ep", None),
        P("ep", None, "tp"),
        P("ep", None, "tp"),
        P("ep", "tp", None),
        P(None, "tp"),
        P(None, "tp"),
        P("tp", None),
    )
    return jax.shard_map(
        functools.partial(local, plane_count(mesh)),
        mesh=mesh,
        in_specs=placed,
        out_specs=(
            P("ep", "tp"),
            P("ep", None),
            P("ep", None, "tp"),
            P("ep", None, "tp"),
            P("ep", "tp", None),
            P("ep", "tp"),
            P("ep", "tp"),
            P("tp", "ep"),
            P("ep", None),
            P("ep", None),
            P("ep", "tp"),
            P("ep"),
            P("ep"),
            P("tp"),
        ),
        check_vma=False,
    )
```

```python
import functools
import math

import jax
import jax.numpy as jnp
from jax import lax
from jax.experimental import pallas as pl
from jax.experimental.pallas import tpu as pltpu
from jax.sharding import PartitionSpec as P

BF16 = jnp.bfloat16
F32 = jnp.float32
LAST = (((1,), (1,)), ((), ()))
FIRST = (((0,), (0,)), ((), ()))


def silu_parts(pre):
    sigmoid = jax.nn.sigmoid(pre)
    return (pre * sigmoid, sigmoid * (1.0 + pre * (1.0 - sigmoid)))


def dot(left, right):
    return jnp.dot(left, right, preferred_element_type=F32)


def dot_last(left, right):
    return lax.dot_general(left, right, LAST, preferred_element_type=F32)


def dot_first(left, right):
    return lax.dot_general(left, right, FIRST, preferred_element_type=F32)


def row_sums(values):
    ones = jnp.ones((8, values.shape[1]), F32)
    sums = lax.dot_general(
        ones, values, LAST, precision=lax.Precision.HIGHEST, preferred_element_type=F32
    )
    return sums[:1]


def plane_count(mesh):
    count = mesh.shape["ep"]
    try:
        planes = len({tuple(d.coords)[2] for d in mesh.devices.flat})
    except (AttributeError, TypeError, IndexError):
        planes = 0
    if planes < 1 or count % planes:
        planes = max(d for d in range(1, math.isqrt(count) + 1) if count % d == 0)
    return planes


def copy_to(src, dst, send, recv, ep, tp):
    return pltpu.make_async_remote_copy(
        src_ref=src,
        dst_ref=dst,
        send_sem=send,
        recv_sem=recv,
        device_id=(ep, tp),
        device_id_type=pl.DeviceIdType.MESH,
    )


def layer_kernel(
    planes, width, cap,
    ids, gates, tokens, cotangent, wg_in, wu_in, wd_in, sg_in, su_in, sd_in,
    tok_out, gate_out, gg_out, gu_out, gd_out, sg_out, su_out, sd_out,
    gn_out, un_out, dn_out, sgn_out, sun_out, sdn_out,
    toks, cots, own_table, line_table, ready, land_t, land_c,
    w_g, w_u, w_d, s_g, s_u, s_d,
    hid, dgate, dup, act, slant, tp_in, ret_in, z_out, z_in, routed,
    stage_g, stage_u, stage_d, acc_g, acc_u, acc_d,
    deal_gu, deal_d, deal_gu_in, deal_d_in, sh_part, sh_in,
    gate_part, gate_in, gate_sum, gate_back, norm_part, norm_in, sdn_part, sdn_in,
    tok_done, gate_done, sg_done, su_done, sd_done, gn_done, un_done, dn_done, sgn_done, sun_done, sdn_done,
    load_sem, table_sem, line_sem, share_sem, plane_sem, pair_sem, tp_sem, ret_sem, z_sem,
    deal_sem, misc_sem, pair_gate_sem, gate_sem, sdn_sem, stage_sem, out_sem,
):
    me, core = lax.axis_index("ep"), lax.axis_index("tp")
    z, q = me // width, me % width
    experts = planes * width
    rows, model = tokens.shape
    cols = model // 2
    hidden = w_g.shape[1]
    slots = width * cap
    take = model // experts
    span = width * take
    mine = pl.ds(pl.multiple_of(core * cols, cols), cols)
    other = pl.ds(pl.multiple_of((1 - core) * cols, cols), cols)
    parts = (toks, cots)
    lands = (land_t, land_c)

    def landed(ref, sem):
        copy_to(ref, ref, sem, sem, me, 1 - core).wait_recv()

    def sent(ref, sem):
        copy_to(ref, ref, sem, sem, me, 1 - core).wait_send()

    loads = [
        pltpu.make_async_copy(src, dst, load_sem.at[i])
        for i, (src, dst) in enumerate(
            (
                (tokens, toks.at[z]),
                (cotangent, cots.at[z]),
                (sg_in, s_g),
                (su_in, s_u),
                (sd_in, s_d),
                (wg_in, w_g),
                (wu_in, w_u),
                (wd_in, w_d),
            )
        )
    ]
    for load in loads[:2]:
        load.start()
    flushed = []
    barrier = pltpu.get_barrier_semaphore()

    def greet(ep, tp):
        pl.semaphore_signal(
            barrier, inc=1, device_id=(ep, tp), device_id_type=pl.DeviceIdType.MESH
        )

    def greet_peer(step, carry):
        greet((me + step) % experts, core)
        return carry

    greet(me, 1 - core)
    lax.fori_loop(1, experts, greet_peer, 0)

    def flush(src, dst):
        copy = pltpu.make_async_copy(src, dst, out_sem.at[len(flushed)])
        copy.start()
        flushed.append(copy)

    def onward(way):
        there = z + 1 - 2 * way
        return (there >= 0) & (there < planes)

    def line_copy(way, block, part, source=None):
        there = jnp.clip(z + 1 - 2 * way, 0, planes - 1)
        ref = parts[part].at[block, :, mine]
        return copy_to(
            ref if source is None else source,
            ref,
            line_sem.at[0, way, block, part],
            line_sem.at[1, way, block, part],
            there * width + q,
            core,
        )

    def line_start(part, source):
        for way in range(2):

            @pl.when(onward(way))
            def _():
                line_copy(way, z, part, source.at[:, mine]).start()

    named = lax.broadcasted_iota(jnp.int32, (experts, rows), 0)
    names, gate_of = jnp.zeros((experts, rows), F32), jnp.zeros((experts, rows), F32)
    for k in range(ids.shape[0]):
        same = named == ids[k : k + 1, :]
        names = names + jnp.where(same, 1.0, 0.0)
        gate_of = gate_of + jnp.where(same, gates[k : k + 1, :], 0.0)
    before = lax.broadcasted_iota(jnp.int32, (rows, rows), 0) < lax.broadcasted_iota(jnp.int32, (rows, rows), 1)
    rank = dot(names.astype(BF16), jnp.where(before, 1.0, 0.0).astype(BF16))
    rank = jnp.where(names > 0.0, rank, -1.0)
    for e in range(experts):
        own_table[e // width, 0, e % width] = rank[e : e + 1, :]
        own_table[e // width, 1, e % width] = gate_of[e : e + 1, :]
    line_table[z] = own_table[z]
    pl.semaphore_wait(barrier, experts)
    line_start(0, tokens)

    def table_copy(step):
        there = (z + step) % planes
        return copy_to(
            own_table.at[there], line_table.at[z], table_sem.at[0, step - 1], table_sem.at[1, step - 1],
            there * width + q, core,
        )

    for step in range(1, planes):
        table_copy(step).start()
    line_start(1, cotangent)

    def share_copy(block, part):
        ref = parts[part].at[block, :, mine]
        return copy_to(ref, ref, share_sem.at[0, block, part], share_sem.at[1, block, part], me, 1 - core)

    def plane_copy(block, d, part):
        to_q = (q + d) % width
        return copy_to(
            ready.at[block, part, to_q],
            lands[part].at[block, q, :, mine],
            plane_sem.at[0, block, d, part],
            plane_sem.at[1, block, d, part],
            z * width + to_q,
            core,
        )

    def pair_copy(block, d, part):
        ref = lands[part].at[block, (q + width - d) % width, :, mine]
        return copy_to(
            ref, ref, pair_sem.at[0, block, d, part], pair_sem.at[1, block, d, part], me, 1 - core
        )

    def tp_copy(block):
        return copy_to(
            ready.at[block, 1 - core], tp_in.at[block], tp_sem.at[0, block], tp_sem.at[1, block],
            me, 1 - core,
        )

    def ret_copy(block, d):
        to_q = (q + d) % width
        return copy_to(
            tp_in.at[block, to_q], ret_in.at[block, q], ret_sem.at[0, block, d], ret_sem.at[1, block, d],
            z * width + to_q, core,
        )

    def z_copy(block):
        return copy_to(
            z_out.at[block], z_in.at[z], z_sem.at[0, block], z_sem.at[1, z], block * width + q, core
        )

    def hits(block):
        ranks = line_table[block, 0]
        at = lax.broadcasted_iota(jnp.int32, (width, cap, rows), 1).astype(F32)
        return (at == ranks).reshape(slots, rows)

    inner = jnp.where(2 * z <= planes - 1, 1, 0)

    def each(step, act, ranks=(0, 2)):
        def one(rank, carry):
            way = inner + rank - 2 * inner * rank
            block = z - step + 2 * step * way
            valid = (step >= 0) & (block >= 0) & (block < planes) & ((step > 0) | (rank == 0))

            @pl.when(valid)
            def _():
                act(jnp.clip(block, 0, planes - 1), way)

            return carry

        lax.fori_loop(*ranks, one, 0)

    def select(part, block):
        hit = hits(block)
        picked = dot(jnp.where(hit, 1.0, 0.0).astype(BF16), parts[part][block, :, mine])
        if part == 1:
            gate_of = jnp.broadcast_to(line_table[block, 1], (width, cap, rows)).reshape(slots, rows)
            picked = picked * jnp.sum(jnp.where(hit, gate_of, 0.0), axis=1, keepdims=True)
        ready[block, part] = picked.astype(BF16).reshape(width, cap, cols)

        def one(d, carry):
            plane_copy(block, d, part).start()
            return carry

        lax.fori_loop(1, width, one, 0)
        lands[part][block, q, :, mine] = ready[block, part, q]
        pair_copy(block, 0, part).start()

    def pass_on(part, block):
        def one(d, carry):
            landed(lands[part].at[block, q, :, mine], plane_sem.at[1, block, d, part])
            pair_copy(block, d, part).start()
            return carry

        lax.fori_loop(1, width, one, 0)

    def paired(part, block):
        def one(d, carry):
            landed(lands[part].at[block, (q + width - d) % width, :, other], pair_sem.at[1, block, d, part])
            return carry

        lax.fori_loop(0, width, one, 0)

        def freed(d, carry):
            sent(ready.at[block, part, 0], plane_sem.at[0, block, d, part])
            return carry

        lax.fori_loop(1, width, freed, 0)

    def shared(block, way):
        for part in range(2):

            @pl.when(block != z)
            def _():
                landed(parts[part].at[block, :, other], share_sem.at[1, block, part])

        gate_pre = dot(toks[block], s_g[...])
        up_pre = dot(toks[block], s_u[...])
        active, slope = silu_parts(gate_pre)
        h = (active * up_pre).astype(BF16)
        h_cot = dot_last(cots[block], s_d[...])
        d_gate = (h_cot * up_pre * slope).astype(BF16)
        d_up = (h_cot * active).astype(BF16)
        here = pl.ds(pl.multiple_of(z * span, span), span)
        acc_g[...] += dot_first(toks[block, :, here], d_gate)
        acc_u[...] += dot_first(toks[block, :, here], d_up)
        acc_d[...] += dot_first(h, cots[block, :, here])

        @pl.when(block == z)
        def _():
            wide = cols // 2

            def one(i, carry):
                at = pl.ds(pl.multiple_of(i * wide, wide), wide)
                sh_part[:, at] = (dot_last(d_gate, s_g[at, :]) + dot_last(d_up, s_u[at, :])).astype(BF16)
                return carry

            lax.fori_loop(0, model // wide, one, 0)
            sh_copy.start()

    sh_copy = copy_to(sh_part.at[:, other], sh_in, misc_sem.at[0, 0], misc_sem.at[1, 0], me, 1 - core)

    def compute(last, block):
        paired(0, block)
        inputs = land_t[block].reshape(slots, model)
        gate_pre = dot(inputs, w_g[...])
        up_pre = dot(inputs, w_u[...])
        active, slope = silu_parts(gate_pre)
        act[...] = active
        slant[...] = up_pre * slope
        hid[block] = (active * up_pre).astype(BF16)

        @pl.when(last)
        def _():
            pass_on(1, block)

        paired(1, block)
        h_cot = dot_last(land_c[block].reshape(slots, model), w_d[...])
        d_gate = (h_cot * slant[...]).astype(BF16)
        d_up = (h_cot * act[...]).astype(BF16)
        dgate[block] = d_gate
        dup[block] = d_up
        gate_row = row_sums(hid[block].astype(F32) * h_cot)
        for w in range(width):
            gate_part[block, w, :, :cap] = gate_row[:, w * cap : (w + 1) * cap]
        gate_pair(block).start()
        wide = cols // 2

        def half(which):
            def one(i, carry):
                at = pl.ds(pl.multiple_of(which * cols + i * wide, wide), wide)
                out = dot_last(d_gate, w_g[at, :]) + dot_last(d_up, w_u[at, :])
                here = pl.ds(pl.multiple_of(i * wide, wide), wide)
                ready[block, which, :, :, here] = out.astype(BF16).reshape(width, cap, wide)
                return carry

            lax.fori_loop(0, 2, one, 0)

        def one(i, carry):
            half((1 - core) * (1 - i) + core * i)

            @pl.when(i == 0)
            def _():
                tp_copy(block).start()

            return carry

        lax.fori_loop(0, 2, one, 0)

    def gate_pair(block):
        return copy_to(
            gate_part.at[block], gate_in.at[block], pair_gate_sem.at[0, block], pair_gate_sem.at[1, block],
            me, 1 - core,
        )

    def gate_copy(block, d):
        to_q = (q + d) % width
        return copy_to(
            gate_sum.at[block, to_q], gate_back.at[me], gate_sem.at[0, block, d], gate_sem.at[1, z, d],
            block * width + to_q, core,
        )

    def gate_sends(block, way):
        gate_pair(block).wait_recv()
        gate_sum[block] = gate_part[block] + gate_in[block]

        def one(d, carry):
            @pl.when((block != z) | (d > 0))
            def _():
                gate_copy(block, d).start()

            return carry

        lax.fori_loop(0, width, one, 0)

        @pl.when(block == z)
        def _():
            gate_back[me] = gate_sum[z, q]

    def sums(block, way):
        landed(tp_in.at[block], tp_sem.at[1, block])
        tp_in[block] = (ready[block, core].astype(F32) + tp_in[block].astype(F32)).astype(BF16)

        def one(d, carry):
            ret_copy(block, d).start()
            return carry

        lax.fori_loop(1, width, one, 0)
        ret_in[block, q] = tp_in[block, q]

    def scatter(block, way):
        def one(d, carry):
            landed(ret_in.at[block, q], ret_sem.at[1, block, d])
            return carry

        lax.fori_loop(1, width, one, 0)
        hit = jnp.where(hits(block), 1.0, 0.0).astype(BF16)
        back = dot_first(hit, ret_in[block].reshape(slots, cols))

        @pl.when(block == z)
        def _():
            routed[...] = back

        @pl.when(block != z)
        def _():
            z_out[block] = back.astype(BF16)
            z_copy(block).start()

    for load in loads[:2]:
        load.wait()
    for load in loads[2:]:
        load.start()
    acc_g[...] = jnp.zeros_like(acc_g)
    acc_u[...] = jnp.zeros_like(acc_u)
    acc_d[...] = jnp.zeros_like(acc_d)
    gate_part[...] = jnp.zeros_like(gate_part)

    def body(step, carry):
        @pl.when(step == 1)
        def _():
            for load in loads[2:]:
                load.wait()
            for other_step in range(1, planes):
                landed(line_table.at[z], table_sem.at[1, other_step - 1])

        def expert(last, block):
            compute(last, block)

            @pl.when(block != z)
            def _():
                sums(block, 0)

            gate_sends(block, 0)

        def ahead(block, way):
            pass_on(0, block)
            pass_on(1, block)
            expert(False, block)

        early = (step == 2) & between
        edge = (step < planes) & jnp.logical_not(between)

        @pl.when(early)
        def _():
            each(1, ahead, (0, 1))

        for part in range(2):

            def arrive(block, way):
                @pl.when(step > 0)
                def _():
                    landed(parts[part].at[block, :, mine], line_sem.at[1, way, block, part])

                    @pl.when(onward(way))
                    def _():
                        line_copy(way, block, part).start()

                    share_copy(block, part).start()

            each(step, arrive)
            each(step, lambda block, way: select(part, block), (0, 1))
            if part == 0:

                @pl.when(edge)
                def _():
                    each(step - 1, ahead, (0, 1))

        def select_both(block, way):
            for part in range(2):
                select(part, block)

        each(step, select_both, (1, 2))
        last = step > jnp.maximum(z, planes - 1 - z)
        start = jnp.where(early | edge, 1, 0)

        @pl.when(step > 2)
        def _():
            each(step - 2, scatter, (0, 1))

        @pl.when((step == planes) & jnp.logical_not(between))
        def _():
            sums(z, 0)

        def hand_on(block, way):
            pass_on(0, block)

            @pl.when(jnp.logical_not(last))
            def _():
                pass_on(1, block)

        each(step - 1, hand_on, (start, 2))
        each(step - 1, shared)

        each(step - 1, lambda block, way: expert(last, block), (start, 2))

        @pl.when(step > 2)
        def _():
            each(step - 2, scatter, (1, 2))

        return carry

    between = (z > 0) & (z < planes - 1)
    lax.fori_loop(0, planes + 1, body, 0)

    for p in range(width):
        at = slice(p * take, (p + 1) * take)
        deal_gu[p, 0] = acc_g[at, :].astype(BF16)
        deal_gu[p, 1] = acc_u[at, :].astype(BF16)
        deal_d[p] = acc_d[:, at].astype(BF16)

    def deal_copies(d):
        to_q = (q + d) % width
        peer = z * width + to_q
        return (
            copy_to(deal_gu.at[to_q], deal_gu_in.at[d], deal_sem.at[0, d, 0], deal_sem.at[1, d, 0], peer, core),
            copy_to(deal_d.at[to_q], deal_d_in.at[d], deal_sem.at[0, d, 1], deal_sem.at[1, d, 1], peer, core),
        )

    def deal(d, carry):
        for copy in deal_copies(d):
            copy.start()
        return carry

    lax.fori_loop(1, width, deal, 0)

    @pl.when(between)
    def _():
        sums(z, 0)

    wide = stage_g.shape[1]
    chunks = model // wide

    def stage_copies(i, slot):
        at = pl.ds(pl.multiple_of(i * wide, wide), wide)
        return (
            pltpu.make_async_copy(stage_g.at[slot], gg_out.at[at, :], stage_sem.at[slot, 0]),
            pltpu.make_async_copy(stage_u.at[slot], gu_out.at[at, :], stage_sem.at[slot, 1]),
            pltpu.make_async_copy(stage_d.at[slot], gd_out.at[:, at], stage_sem.at[slot, 2]),
        )

    dn_done[...] = jnp.zeros_like(dn_done)
    norm_part[...] = jnp.zeros_like(norm_part)

    def sdn_copy(step):
        return copy_to(
            sdn_part, sdn_in.at[me], sdn_sem.at[0, step], sdn_sem.at[1, step], (me + step) % experts, core
        )

    def deal_finish():
        def deal_done(d, carry):
            for copy in deal_copies(d):
                copy.wait_recv()
            return carry

        lax.fori_loop(1, width, deal_done, 0)
        grad_g, grad_u, grad_d = deal_gu[q, 0].astype(F32), deal_gu[q, 1].astype(F32), deal_d[q].astype(F32)
        for d in range(1, width):
            grad_g = grad_g + deal_gu_in[d, 0].astype(F32)
            grad_u = grad_u + deal_gu_in[d, 1].astype(F32)
            grad_d = grad_d + deal_d_in[d].astype(F32)
        sg_done[...] = grad_g
        su_done[...] = grad_u
        sd_done[...] = grad_d
        norm_part[2:3, :take] = row_sums(grad_g * grad_g)
        norm_part[3:4, :take] = row_sums(grad_u * grad_u)
        sdn_part[...] = row_sums(grad_d * grad_d)
        sdn_in[me] = sdn_part[...]

        def send_sdn(step, carry):
            sdn_copy(step).start()
            return carry

        lax.fori_loop(1, experts, send_sdn, 0)

    def weight_grads(i, carry):
        slot = i % 2
        at = pl.ds(pl.multiple_of(i * wide, wide), wide)

        @pl.when(i >= 2)
        def _():
            for copy in stage_copies(i - 2, slot):
                copy.wait()

        block_rows = land_t[:, :, :, at].reshape(planes * slots, wide)
        grad = dot_first(block_rows, dgate[...].reshape(planes * slots, hidden))
        stage_g[slot] = grad
        norm_part[0:1, at] = row_sums(grad * grad)
        grad = dot_first(block_rows, dup[...].reshape(planes * slots, hidden))
        stage_u[slot] = grad
        norm_part[1:2, at] = row_sums(grad * grad)
        block_rows = land_c[:, :, :, at].reshape(planes * slots, wide)
        grad = dot_first(hid[...].reshape(planes * slots, hidden), block_rows)
        stage_d[slot] = grad
        dn_done[...] += row_sums(grad * grad)
        for copy in stage_copies(i, slot):
            copy.start()

        @pl.when(i == chunks // 2)
        def _():
            each(planes - 1, scatter)

        @pl.when(i == max(chunks - 2, chunks // 2))
        def _():
            deal_finish()

        return carry

    lax.fori_loop(0, chunks, weight_grads, 0)
    flush(dn_done, dn_out)

    flush(sg_done, sg_out)
    flush(su_done, su_out)
    flush(sd_done, sd_out)
    norm_pair = copy_to(norm_part, norm_in, misc_sem.at[0, 2], misc_sem.at[1, 2], me, 1 - core)
    norm_pair.start()

    def gate_arrived(source, carry):
        def one(d, inner):
            @pl.when((source != z) | (d > 0))
            def _():
                landed(gate_back.at[me], gate_sem.at[1, source, d])

            return inner

        return lax.fori_loop(0, width, one, carry)

    lax.fori_loop(0, planes, gate_arrived, 0)
    top, lanes = ids.shape[0], gate_back.shape[2]

    def gate_rows(e, total):
        at = lax.broadcasted_iota(jnp.int32, (lanes, rows), 0).astype(F32)
        hit = jnp.where(at == own_table[e // width, 0, e % width], 1.0, 0.0)
        back = lax.dot_general(
            jnp.broadcast_to(gate_back[e], (8, lanes)), hit, (((1,), (0,)), ((), ())),
            precision=lax.Precision.HIGHEST, preferred_element_type=F32,
        )
        return total + jnp.where(ids[...] == e, jnp.broadcast_to(back[:1], (top, rows)), 0.0)

    total = lax.fori_loop(0, experts, gate_rows, jnp.zeros((top, rows), F32))
    gate_done[...] = total / gates[...]
    flush(gate_done, gate_out)

    norm_pair.wait_recv()
    total = norm_part[...] + norm_in[...]
    gn_done[...] = total[0:1]
    un_done[...] = total[1:2]
    sgn_done[...] = total[2:3, :take]
    sun_done[...] = total[3:4, :take]
    flush(gn_done, gn_out)
    flush(un_done, un_out)
    flush(sgn_done, sgn_out)
    flush(sun_done, sun_out)

    scatter(z, 0)
    sh_copy.wait_recv()
    routed[...] += sh_part[:, mine].astype(F32) + sh_in[...].astype(F32)

    def gather(step, carry):
        source = (z + step) % planes
        landed(z_in.at[source], z_sem.at[1, source])
        routed[...] += z_in[source].astype(F32)
        return carry

    lax.fori_loop(1, planes, gather, 0)
    tok_done[...] = routed[...].astype(BF16)
    flush(tok_done, tok_out)

    def small_done(step, carry):
        sdn_copy(step).wait()
        return carry

    lax.fori_loop(1, experts, small_done, 0)
    sdn_done[...] = jnp.sum(sdn_in[...], axis=0)
    flush(sdn_done, sdn_out)
    for i in range(max(chunks - 2, 0), chunks):
        for copy in stage_copies(i, i % 2):
            copy.wait()
    for step in range(1, planes):
        table_copy(step).wait_send()
    sh_copy.wait_send()
    norm_pair.wait_send()

    def deal_sent(d, carry):
        for copy in deal_copies(d):
            copy.wait_send()
        return carry

    lax.fori_loop(1, width, deal_sent, 0)

    def drain(block, carry):
        for part in range(2):
            for way in range(2):
                behind = (block <= z) if way == 0 else (block >= z)

                @pl.when(behind & onward(way))
                def _():
                    sent(parts[part].at[block, :, mine], line_sem.at[0, way, block, part])

            @pl.when(block != z)
            def _():
                share_copy(block, part).wait_send()

            def pairs(d, inner):
                pair_copy(block, d, part).wait_send()
                return inner

            lax.fori_loop(0, width, pairs, 0)
        tp_copy(block).wait_send()
        gate_pair(block).wait_send()

        def gate_sent(d, inner):
            @pl.when((block != z) | (d > 0))
            def _():
                gate_copy(block, d).wait_send()

            return inner

        lax.fori_loop(0, width, gate_sent, 0)

        def returns(d, inner):
            ret_copy(block, d).wait_send()
            return inner

        lax.fori_loop(1, width, returns, 0)

        @pl.when(block != z)
        def _():
            z_copy(block).wait_send()

        return carry

    lax.fori_loop(0, planes, drain, 0)
    for copy in flushed:
        copy.wait()


def finish_kernel(count, *refs):
    sources, results, held = refs[:count], refs[count : 2 * count], refs[2 * count : 3 * count]
    in_sem, out_sem = refs[3 * count :]
    moves = []
    for i in range(count):
        rows = sources[i].shape[0]
        pieces = 4 if rows % 32 == 0 and sources[i].shape[1] * rows >= 2**18 else 1
        step = rows // pieces
        for p in range(pieces):
            at = slice(p * step, (p + 1) * step)
            moves.append(
                (
                    pltpu.make_async_copy(sources[i].at[at], held[i].at[at], in_sem.at[i, p]),
                    pltpu.make_async_copy(held[i].at[at], results[i].at[at], out_sem.at[i, p]),
                )
            )
    for taken, _ in moves:
        taken.start()
    for taken, given in moves:
        taken.wait()
        given.start()
    for _, given in moves:
        given.wait()


def finish(arrays):
    count = len(arrays)
    hbm = pl.BlockSpec(memory_space=pltpu.HBM)
    return pl.pallas_call(
        functools.partial(finish_kernel, count),
        out_shape=[jax.ShapeDtypeStruct(a.shape, a.dtype) for a in arrays],
        in_specs=[hbm] * count,
        out_specs=[hbm] * count,
        scratch_shapes=[pltpu.VMEM(a.shape, a.dtype) for a in arrays]
        + [pltpu.SemaphoreType.DMA((count, 4)), pltpu.SemaphoreType.DMA((count, 4))],
        compiler_params=pltpu.CompilerParams(vmem_limit_bytes=67043328),
        name="finish",
    )(*arrays)


def layer(planes, cap, ids, gates, tokens, cotangent, w_gate, w_up, w_down, sh_gate, sh_up, sh_down):
    experts = lax.axis_size("ep")
    width = experts // planes
    rows, model = tokens.shape
    lanes = -(-cap // 128) * 128
    cols, hidden = model // 2, w_gate.shape[1]
    take = model // experts
    span = width * take
    slots = width * cap
    wide = min(256, model)
    vmem = pl.BlockSpec(memory_space=pltpu.VMEM)
    hbm = pl.BlockSpec(memory_space=pltpu.HBM)
    out = jax.ShapeDtypeStruct
    dma = pltpu.SemaphoreType.DMA
    far = max(planes - 1, 1)
    return pl.pallas_call(
        functools.partial(layer_kernel, planes, width, cap),
        out_shape=(
            out((rows, cols), BF16),
            out(gates.shape, F32),
            out((model, hidden), F32),
            out((model, hidden), F32),
            out((hidden, model), F32),
            out((take, hidden), F32),
            out((take, hidden), F32),
            out((hidden, take), F32),
            out((1, model), F32),
            out((1, model), F32),
            out((1, hidden), F32),
            out((1, take), F32),
            out((1, take), F32),
            out((1, hidden), F32),
        ),
        in_specs=[vmem] * 2 + [hbm] * 8,
        out_specs=(hbm,) * 14,
        scratch_shapes=[
            pltpu.VMEM((planes, rows, model), BF16),
            pltpu.VMEM((planes, rows, model), BF16),
            pltpu.VMEM((planes, 2, width, 1, rows), F32),
            pltpu.VMEM((planes, 2, width, 1, rows), F32),
            pltpu.VMEM((planes, 2, width, cap, cols), BF16),
            pltpu.VMEM((planes, width, cap, model), BF16),
            pltpu.VMEM((planes, width, cap, model), BF16),
            pltpu.VMEM((model, hidden), BF16),
            pltpu.VMEM((model, hidden), BF16),
            pltpu.VMEM((hidden, model), BF16),
            pltpu.VMEM((model, hidden), BF16),
            pltpu.VMEM((model, hidden), BF16),
            pltpu.VMEM((hidden, model), BF16),
            pltpu.VMEM((planes, slots, hidden), BF16),
            pltpu.VMEM((planes, slots, hidden), BF16),
            pltpu.VMEM((planes, slots, hidden), BF16),
            pltpu.VMEM((slots, hidden), F32),
            pltpu.VMEM((slots, hidden), F32),
            pltpu.VMEM((planes, width, cap, cols), BF16),
            pltpu.VMEM((planes, width, cap, cols), BF16),
            pltpu.VMEM((planes, rows, cols), BF16),
            pltpu.VMEM((planes, rows, cols), BF16),
            pltpu.VMEM((rows, cols), F32),
            pltpu.VMEM((2, wide, hidden), F32),
            pltpu.VMEM((2, wide, hidden), F32),
            pltpu.VMEM((2, hidden, wide), F32),
            pltpu.VMEM((span, hidden), F32),
            pltpu.VMEM((span, hidden), F32),
            pltpu.VMEM((hidden, span), F32),
            pltpu.VMEM((width, 2, take, hidden), BF16),
            pltpu.VMEM((width, hidden, take), BF16),
            pltpu.VMEM((width, 2, take, hidden), BF16),
            pltpu.VMEM((width, hidden, take), BF16),
            pltpu.VMEM((rows, model), BF16),
            pltpu.VMEM((rows, cols), BF16),
            pltpu.VMEM((planes, width, 1, lanes), F32),
            pltpu.VMEM((planes, width, 1, lanes), F32),
            pltpu.VMEM((planes, width, 1, lanes), F32),
            pltpu.VMEM((experts, 1, lanes), F32),
            pltpu.VMEM((8, model), F32),
            pltpu.VMEM((8, model), F32),
            pltpu.VMEM((1, hidden), F32),
            pltpu.VMEM((experts, 1, hidden), F32),
            pltpu.VMEM((rows, cols), BF16),
            pltpu.VMEM(gates.shape, F32),
            pltpu.VMEM((take, hidden), F32),
            pltpu.VMEM((take, hidden), F32),
            pltpu.VMEM((hidden, take), F32),
            pltpu.VMEM((1, model), F32),
            pltpu.VMEM((1, model), F32),
            pltpu.VMEM((1, hidden), F32),
            pltpu.VMEM((1, take), F32),
            pltpu.VMEM((1, take), F32),
            pltpu.VMEM((1, hidden), F32),
            dma((8,)),
            dma((2, far)),
            dma((2, 2, planes, 2)),
            dma((2, planes, 2)),
            dma((2, planes, width, 2)),
            dma((2, planes, width, 2)),
            dma((2, planes)),
            dma((2, planes, width)),
            dma((2, planes)),
            dma((2, width, 2)),
            dma((2, 3)),
            dma((2, planes)),
            dma((2, planes, width)),
            dma((2, experts)),
            dma((2, 3)),
            dma((16,)),
        ],
        compiler_params=pltpu.CompilerParams(collective_id=0, has_side_effects=True, vmem_limit_bytes=67043328),
        name="layer",
    )(ids, gates, tokens, cotangent, w_gate, w_up, w_down, sh_gate, sh_up, sh_down)


def local(planes, tokens, expert_ids, gates, cotangent, w_gate, w_up, w_down, sh_gate, sh_up, sh_down):
    experts = lax.axis_size("ep")
    rows, top_count = expert_ids.shape
    capacity = 3 * rows * top_count // (2 * experts)
    cap = -(-capacity // 8) * 8
    arrays = layer(
        planes, cap, expert_ids.T, gates.T, tokens, cotangent,
        w_gate[0], w_up[0], w_down[0], sh_gate, sh_up, sh_down,
    )
    (token_grad, gate_grad, grad_g, grad_u, grad_d, out_g, out_u, out_d, gate_norms, up_norms, down_norms,
     shared_gate, shared_up, shared_down) = finish(arrays)
    return (
        token_grad,
        gate_grad.T,
        grad_g[None],
        grad_u[None],
        grad_d[None],
        out_g,
        out_u,
        out_d,
        gate_norms,
        up_norms,
        down_norms,
        shared_gate[0],
        shared_up[0],
        shared_down[0],
    )


def solution(mesh):
    placed = (
        P("ep", None),
        P("ep", None),
        P("ep", None),
        P("ep", None),
        P("ep", None, "tp"),
        P("ep", None, "tp"),
        P("ep", "tp", None),
        P(None, "tp"),
        P(None, "tp"),
        P("tp", None),
    )
    return jax.shard_map(
        functools.partial(local, plane_count(mesh)),
        mesh=mesh,
        in_specs=placed,
        out_specs=(
            P("ep", "tp"),
            P("ep", None),
            P("ep", None, "tp"),
            P("ep", None, "tp"),
            P("ep", "tp", None),
            P("ep", "tp"),
            P("ep", "tp"),
            P("tp", "ep"),
            P("ep", None),
            P("ep", None),
            P("ep", "tp"),
            P("ep"),
            P("ep"),
            P("tp"),
        ),
        check_vma=False,
    )
```
